256 devices in a mesh: sp: 16 (over y, x), tp: 16 (over z, core).
Axes of the slice: x: 4, y: 4, z: 8, core: 2. Of those that a mesh axis runs over, the one named last changes fastest.
Arguments:
- upstream: bfloat16 [4096, 4096], P('sp', 'tp'), may hold values from -6 to 6
- stream: bfloat16 [4096, 4096], P('sp', 'tp'), may hold values from -400 to 400
- norm_gain: float32 [4096], P('tp'), may hold values from 0.1 to 1.9
- routes: int32 [4096, 2], P('sp'), may hold values from 0 to 15, all different within a row; in each aligned block of 256 rows (0 to 255, 256 to 511, ...) at most 48 rows name the same one
- route_weights: float32 [4096, 2], P('sp'), may hold values from 0.1 to 1
- w_gate: bfloat16 [16, 4096, 2048], P('sp', None, 'tp'), may hold values from -0.09375 to 0.09375
- w_up: bfloat16 [16, 4096, 2048], P('sp', None, 'tp'), may hold values from -0.09375 to 0.09375
- w_down: bfloat16 [16, 2048, 4096], P('sp', 'tp'), may hold values from -0.125 to 0.125
- value_in: bfloat16 [4096, 2048], P('sp', 'tp'), may hold values from -6 to 6
- gate_in: bfloat16 [4096, 2048], P('sp', 'tp'), may hold values from -6 to 6
- conv_pre: bfloat16 [4096, 2048], P('sp', 'tp'), may hold values from -200 to 200
- ln_gain: float32 [2048], P('tp'), may hold values from 0.1 to 1.9
- conv_taps: float32 [31, 2048], P(None, 'tp'), may hold values from -1 to 1
- w_out: bfloat16 [2048, 4096], P('tp'), may hold values from -0.125 to 0.125
Outputs:
- grad_gate: float32 [16, 4096, 2048], P('sp', None, 'tp')
- grad_up: float32 [16, 4096, 2048], P('sp', None, 'tp')
- grad_down: float32 [16, 2048, 4096], P('sp', 'tp')
- grad_out: float32 [2048, 4096], P('tp', 'sp')
- value_grad: bfloat16 [4096, 2048], P('sp', 'tp')
- gate_grad: bfloat16 [4096, 2048], P('sp', 'tp')
The draws below stay inside these ranges and needn't reach their ends.
Inputs may be any that keep to these rules, and one draw needn't show every extreme that they name: `routes`: each token names two different experts. Among the tokens of one index of sp no expert is named more than 48 times, and in every draw some expert exactly 48 times.
All inputs are finite; a program needn't handle non-finite values.
Results may differ from the reference program's by a relative error of at most 0.0071.
Values may be sent and summed in bfloat16 or wider, within the bound.
A program may use at most 128 MiB of HBM per device.

```python
import math
import jax
import jax.numpy as jnp
import numpy as np
from jax import lax

D = 4096
C = 2048
FF = 2048
TAPS = 31
TOK_DEV = 256
TOKENS = 4096
EXPERTS = 16
CAP = 48
N_SP = 16


def draw_stream(key, part):
    subkeys = jax.random.split(jax.random.fold_in(key, 11), 3)
    random_part = jnp.clip(jax.random.normal(subkeys[0], (TOKENS, D), jnp.float32), -6.0, 6.0)
    row_scale = jnp.exp(jax.random.uniform(subkeys[1], (TOKENS, 1), jnp.float32, 0.0, math.log(10.0)))
    rising = jnp.exp(math.log(10.0) * (jnp.arange(D, dtype=jnp.float32) + 0.5) / D)
    jitter = jnp.exp(jax.random.uniform(subkeys[2], (D,), jnp.float32, -0.3, 0.3))
    column_scale = rising * jitter
    return (random_part * row_scale * column_scale[None, :] / 3.0).astype(jnp.bfloat16)


def draw_conv_pre(key, part):
    subkeys = jax.random.split(jax.random.fold_in(key, 23), 4)
    random_part = jnp.clip(jax.random.normal(subkeys[0], (TOKENS, C), jnp.float32), -6.0, 6.0)
    row_scale = jnp.exp(jax.random.uniform(subkeys[1], (TOKENS, 1), jnp.float32, 0.0, math.log(4.0)))
    rising = jnp.exp(math.log(10.0) * (jnp.arange(C, dtype=jnp.float32) + 0.5) / C)
    jitter = jnp.exp(jax.random.uniform(subkeys[2], (C,), jnp.float32, -0.3, 0.3))
    column_scale = rising * jitter
    row_offset = 1.5 * jnp.clip(jax.random.normal(subkeys[3], (TOKENS, 1), jnp.float32), -3.0, 3.0)
    return ((random_part * column_scale[None, :] / 3.0 + row_offset) * row_scale).astype(jnp.bfloat16)


def with_spikes(entries, rng, source, target, blocks, factor):
    def block_of(position):
        return (jnp.arange(entries.shape[position]) // (entries.shape[position] // blocks)).reshape((-1,) + (1,) * (entries.ndim - 1 - position))

    first = jax.random.permutation(rng, blocks)[block_of(target)]
    other_side = (block_of(target) + blocks // 2) % blocks
    return jnp.where((block_of(source) == first) | (block_of(source) == other_side), factor * entries, entries)


def block_levels(own_key, dims, pieces, low, top_value):
    def one(position, blocks):
        draws = jax.random.uniform(jax.random.fold_in(jax.random.fold_in(own_key, 6), position), (blocks,), jnp.float32, low / len(pieces), top_value / len(pieces))
        return jnp.repeat(jnp.exp(draws), dims[position] // blocks).reshape((-1,) + (1,) * (len(dims) - position - 1))

    gain = one(*pieces[0])
    for cut in pieces[1:]:
        gain = gain * one(*cut)
    return gain


def assign_block(key, own, number, rows, count, top, reach, slope):
    sequence = jax.random.permutation(key, count)
    packed, common = shares(count, rows * top, reach, slope, True), shares(count, rows * top, reach, slope, False)
    places = jnp.arange(count)

    def named(sizes, turn):
        used = int((sizes > 0).sum())
        fixed = max(1, used // 4)
        shifted = fixed + (places - fixed + turn * (used - fixed)) % max(1, count - fixed)
        return jnp.zeros((count,), jnp.int32).at[sequence[jnp.where(places < fixed, places, shifted)]].set(jnp.asarray(sizes, jnp.int32))

    sizes = jnp.where(number % 4 == 0, named(packed, number // 4), named(common, number - number // 4 - 1))
    mixed = jax.random.permutation(jax.random.fold_in(own, 3), count)
    source_of, receiver = mixed[0:count // 2 * 2:2], mixed[1:count // 2 * 2:2]
    room = jnp.minimum(sizes[source_of] - 1, reach - sizes[receiver]) // 2
    room = jnp.where((source_of == sequence[0]) | (receiver == sequence[0]) | (sizes[receiver] == 0), 0, jnp.maximum(room, 0))
    shifted = jax.random.randint(jax.random.fold_in(own, 4), (count // 2,), 0, 1 << 20) % (room + 1)
    sizes = sizes.at[source_of].add(-shifted).at[receiver].add(shifted)
    labels = jnp.searchsorted(jnp.cumsum(sizes), jnp.arange(rows * top), side="right").astype(jnp.int32)
    listing = labels.reshape(top, rows).T
    listing = listing[jax.random.permutation(jax.random.fold_in(own, 1), rows)]
    turn = jax.random.randint(jax.random.fold_in(own, 2), (rows, 1), 0, top)
    return jnp.take_along_axis(listing, (jnp.arange(top)[None, :] + turn) % top, axis=1)


def shares(number_of, total, reach, lean, full):
    loads = [(1 << 20) // math.isqrt(grade ** lean) + 1 for grade in range(1, number_of + 1)]
    largest = reach if full else min(reach, max(-(-total // number_of), total * loads[0] // sum(loads)))
    least = 1 if total - largest >= number_of - 1 else 0
    holding, rest = [largest] + [least] * (number_of - 1), total - largest - least * (number_of - 1)
    while rest > 0:
        candidates = [i for i in range(1, number_of) if holding[i] < largest] or [i for i in range(1, number_of) if holding[i] < reach]
        whole, left = sum([loads[i] for i in candidates]), rest
        for i in candidates:
            addition = min(reach - holding[i], max(1, left * loads[i] // whole), rest)
            holding[i] = holding[i] + addition
            rest = rest - addition
    return np.array(holding)


def scatter_about(own_key, extent, width, limit, pieces=(), kind=jnp.bfloat16):
    values = jax.random.normal(own_key, extent, jnp.float32) * width
    if len(pieces) > 0:
        values = block_levels(own_key, extent, pieces, -0.22, 0.18) * values
    return jnp.clip(values, min=-limit, max=limit).astype(kind)


def bell_draw_with(own_key, extent, scale, most, cuts, heavy, held_as=jnp.bfloat16):
    drawn = scale * jax.random.normal(own_key, extent, jnp.float32)
    if cuts:
        drawn = drawn * block_levels(own_key, extent, cuts, -0.22, 0.18)
    return jnp.clip(with_spikes(drawn, jax.random.fold_in(own_key, 3), *heavy), -most, most).astype(held_as)


def setup_inputs(seed: int = 0) -> dict:
    splits = jax.random.split(jax.random.key(seed), 15)
    upstream = bell_draw_with(splits[0], (TOKENS, D), 1.0, 6.0, ((0, 16), (1, 16)), (0, 1, 16, 2.0))
    stream = draw_stream(jax.random.fold_in(splits[14], 71), 0)
    norm_gain = jnp.clip(1.0 + 0.18 * jax.random.normal(splits[2], (D,), jnp.float32), 0.1, 1.9)
    routes_keys = jax.random.split(jax.random.fold_in(splits[3], 1), TOKENS // TOK_DEV)
    routes_turns = jax.random.permutation(jax.random.fold_in(splits[3], 3), TOKENS // TOK_DEV)
    routes = jax.vmap(lambda own, number: assign_block(jax.random.fold_in(splits[3], 2), own, number, TOK_DEV, EXPERTS, 2, CAP, 1))(routes_keys, routes_turns).reshape((TOKENS, 2))
    route_weights = jnp.clip(jnp.exp(math.log(1.0) - 2.3025851 * jax.random.uniform(splits[4], (TOKENS, 2), jnp.float32) ** block_levels(splits[4], (TOKENS, 2), ((0, 16),), -0.2, 0.2)), 0.1, 1.0)
    w_gate = scatter_about(splits[5], (EXPERTS, D, FF), D ** -0.5, 0.09375, ((0, 16), (2, 16)))
    w_up = scatter_about(splits[6], (EXPERTS, D, FF), D ** -0.5, 0.09375, ((0, 16), (2, 16)))
    w_down = scatter_about(splits[7], (EXPERTS, FF, D), FF ** -0.5, 0.125, ((0, 16), (1, 16)))
    value_in = scatter_about(splits[8], (TOKENS, C), 1.0, 6.0, ((0, 16), (1, 16)))
    gate_in = scatter_about(splits[9], (TOKENS, C), 1.5, 6.0, ((0, 16), (1, 16)))
    conv_pre = draw_conv_pre(jax.random.fold_in(splits[14], 71), 0)
    ln_gain = jnp.clip(1.0 + 0.18 * jax.random.normal(splits[11], (C,), jnp.float32), 0.1, 1.9)
    conv_taps = scatter_about(splits[12], (TAPS, C), TAPS ** -0.5, 1.0, ((1, 16),), jnp.float32)
    w_out = scatter_about(splits[13], (C, D), C ** -0.5, 0.125, ((0, 16),))
    return dict(upstream=upstream, stream=stream, norm_gain=norm_gain, routes=routes, route_weights=route_weights, w_gate=w_gate, w_up=w_up, w_down=w_down, value_in=value_in, gate_in=gate_in, conv_pre=conv_pre, ln_gain=ln_gain, conv_taps=conv_taps, w_out=w_out)


EPSILON = 1e-06

def silu_slope(values):
    logistic = jax.nn.sigmoid(values)
    return logistic * (1.0 + values * (1.0 - logistic))

def reference(upstream, stream, norm_gain, routes, route_weights, w_gate, w_up, w_down, value_in, gate_in, conv_pre, ln_gain, conv_taps, w_out):
    tokens, model_width = stream.shape
    experts = w_gate.shape[0]
    channels = conv_pre.shape[1]
    tap_count = conv_taps.shape[0]
    capacity = 3 * TOK_DEV // N_SP
    expert_rows = N_SP * capacity
    residual = stream.astype(jnp.float32)
    inverse = lax.rsqrt(lax.optimization_barrier(jnp.mean(residual * residual, axis=1, keepdims=True)) + EPSILON)
    normed = (norm_gain[None, :] * residual * inverse).astype(jnp.bfloat16)
    flat_experts = routes.reshape(-1)
    one_hot = (flat_experts[:, None] == jnp.arange(experts, dtype=jnp.int32)[None, :]).astype(jnp.int32)
    blocked = one_hot.reshape(N_SP, 2 * TOK_DEV, experts)
    earlier = (jnp.cumsum(blocked, axis=1) - blocked) * blocked
    slot_rank = lax.optimization_barrier(jnp.sum(earlier, axis=2)).reshape(-1)
    source = jnp.arange(2 * tokens, dtype=jnp.int32) // (2 * TOK_DEV)
    slot_index = flat_experts * expert_rows + source * capacity + slot_rank
    token_of = jnp.full((experts * expert_rows,), tokens, jnp.int32).at[slot_index].set(jnp.arange(2 * tokens, dtype=jnp.int32) // 2)
    weight_of = jnp.zeros((experts * expert_rows,), jnp.float32).at[slot_index].set(route_weights.reshape(-1))
    normed_pad = jnp.concatenate([normed, jnp.zeros((1, model_width), jnp.bfloat16)], axis=0)
    upstream_pad = jnp.concatenate([upstream, jnp.zeros((1, model_width), jnp.bfloat16)], axis=0)

    def one_expert(operands):
        indices, weights, gate_mat, upper_mat, down_mat = operands
        inputs = normed_pad[indices]
        cotangent = (weights[:, None] * upstream_pad[indices].astype(jnp.float32)).astype(jnp.bfloat16)
        gate_pre = jnp.dot(inputs, gate_mat, preferred_element_type=jnp.float32)
        upper_pre = jnp.dot(inputs, upper_mat, preferred_element_type=jnp.float32)
        active = (jax.nn.silu(gate_pre) * upper_pre).astype(jnp.bfloat16)
        active_back = jnp.dot(cotangent, down_mat.T, preferred_element_type=jnp.float32)
        gate_back = (active_back * upper_pre * silu_slope(gate_pre)).astype(jnp.bfloat16)
        upper_back = (active_back * jax.nn.silu(gate_pre)).astype(jnp.bfloat16)
        grad_gate = jnp.dot(inputs.T, gate_back, preferred_element_type=jnp.float32)
        grad_up = jnp.dot(inputs.T, upper_back, preferred_element_type=jnp.float32)
        grad_down = jnp.dot(active.T, cotangent, preferred_element_type=jnp.float32)
        input_back = (jnp.dot(gate_back, gate_mat.T, preferred_element_type=jnp.float32) + jnp.dot(upper_back, upper_mat.T, preferred_element_type=jnp.float32)).astype(jnp.bfloat16)
        return (grad_gate, grad_up, grad_down, input_back)
    grad_gate, grad_up, grad_down, input_back = lax.map(one_expert, (token_of.reshape(experts, expert_rows), weight_of.reshape(experts, expert_rows), w_gate, w_up, w_down))
    token_back = jnp.zeros((tokens + 1, model_width), jnp.float32).at[token_of].add(input_back.reshape(-1, model_width).astype(jnp.float32))[:tokens]
    gained = norm_gain[None, :] * token_back
    inner_sum = lax.optimization_barrier(jnp.sum(gained * residual, axis=1, keepdims=True))
    norm_back = inverse * gained - residual * inverse ** 3 * inner_sum / model_width
    stream_grad = (upstream.astype(jnp.float32) + norm_back).astype(jnp.bfloat16)
    conv_vals = conv_pre.astype(jnp.float32)
    mean_val = lax.optimization_barrier(jnp.mean(conv_vals, axis=1, keepdims=True))
    variance = lax.optimization_barrier(jnp.mean(conv_vals * conv_vals, axis=1, keepdims=True)) - mean_val * mean_val
    inv_std = lax.rsqrt(variance + EPSILON)
    centred = (conv_vals - mean_val) * inv_std
    scaled = centred * ln_gain[None, :]
    mixed_out = jax.nn.silu(scaled).astype(jnp.bfloat16)
    grad_out = jnp.dot(mixed_out.T, stream_grad, preferred_element_type=jnp.float32)
    mixed_back = jnp.dot(stream_grad, w_out.T, preferred_element_type=jnp.float32)
    norm_in = mixed_back * silu_slope(scaled) * ln_gain[None, :]
    conv_back = inv_std * (norm_in - lax.optimization_barrier(jnp.mean(norm_in, axis=1, keepdims=True)) - centred * lax.optimization_barrier(jnp.mean(norm_in * centred, axis=1, keepdims=True)))
    padded = jnp.concatenate([conv_back, jnp.zeros((tap_count - 1, channels), jnp.float32)], axis=0)
    glu_back = jnp.zeros((tokens, channels), jnp.float32)
    for tap_index in range(tap_count):
        offset = tap_count - 1 - tap_index
        glu_back = glu_back + conv_taps[tap_index][None, :] * padded[offset:offset + tokens]
    gate_sigma = jax.nn.sigmoid(gate_in.astype(jnp.float32))
    value_grad = (glu_back * gate_sigma).astype(jnp.bfloat16)
    gate_grad = (glu_back * value_in.astype(jnp.float32) * gate_sigma * (1.0 - gate_sigma)).astype(jnp.bfloat16)
    return (grad_gate, grad_up, grad_down, grad_out, value_grad, gate_grad)
```

```python
import jax
import jax.numpy as jnp
from jax import lax
from jax.experimental import pallas as pl
from jax.experimental.pallas import tpu as pltpu
from jax.sharding import PartitionSpec as P

MESH = pl.DeviceIdType.MESH
F32, BF16 = jnp.float32, jnp.bfloat16
EPSILON = 1e-06
NZ, NS = 8, 16
TOK, W, CH = 256, 256, 128
CAP, ROWS, HALF = 48, 768, 384
MODEL, CHANNELS, TAPS = 4096, 2048, 31
STEPS = ((0, 0), (0, 1), (1, 0), (1, 1))
OFFSETS = (0, 1, -1, 2, -2, 3, -3, 4)


def dot(a, b, ca, cb):
    return lax.dot_general(a, b, (((ca,), (cb,)), ((), ())), preferred_element_type=F32)


def columns_to_rows(columns):
    lane = lax.broadcasted_iota(jnp.int32, (TOK, 128), 1)
    packed = jnp.zeros((TOK, 128), F32)
    for k, column in enumerate(columns):
        packed = jnp.where(lane == k, column, packed)
    return packed.T[0:8, :]


def rows_to_columns(rows):
    return jnp.concatenate([rows, jnp.zeros((120, TOK), F32)], axis=0).T


def silu_slope(values, logistic):
    return logistic * (1.0 + values * (1.0 - logistic))


def comm_kernel(
    gain_ref, routes_ref, rw_ref, lng_ref, up_h, st_h, wg_h, wu_h, wd_h, cp_h, wo_h,
    gg_h, gu_h, gd_h, cb_o, go_o,
    UP, ST, CP, WC, WD, WO, PICK, SW, SI, SC, X, CT, G, A, CAT, ACT, GG, GU, GD,
    SB, SR, RSS, RSR, FIN, RET, SG, MB, MO, CEN, SCL, HS, HALO, GOS, GOR, SS, SX,
    ls, ups, upr, xs, xr, dxs, dxr, as_, ar, cs, cr, dcs, dcr, sbs, sbr, rss, rsr,
    es, er, fs, fr, sgs, sgr, dgs, dgr, gs, gr, hs, hr,
):
    sp = lax.axis_index("sp")
    tp = lax.axis_index("tp")
    z = tp // 2
    c = tp % 2
    sibling = (sp, z * 2 + 1 - c)

    def zat(offset):
        return (z + offset + NZ) % NZ

    def zdev(offset):
        return (sp, zat(offset) * 2 + c)

    def mine(offset):
        return zat(offset) * 2 + c

    def other(offset):
        return zat(offset) * 2 + 1 - c

    def remote(src, dst, ssem, rsem, device):
        return pltpu.make_async_remote_copy(
            src_ref=src, dst_ref=dst, send_sem=ssem, recv_sem=rsem,
            device_id=device, device_id_type=MESH,
        )

    def each_peer(body):
        def step(k, carry):
            body((sp + k) % NS)
            return carry

        lax.fori_loop(1, NS, step, 0)

    barrier = pltpu.get_barrier_semaphore()

    def greet(k, carry):
        pl.semaphore_signal(barrier, inc=1, device_id=(sp, (tp + k) % NS), device_id_type=MESH)
        pl.semaphore_signal(barrier, inc=1, device_id=((sp + k) % NS, tp), device_id_type=MESH)
        return carry

    lax.fori_loop(1, NS, greet, 0)
    loads = [
        pltpu.make_async_copy(up_h, UP.at[z], ls.at[0]),
        pltpu.make_async_copy(st_h, ST, ls.at[1]),
        pltpu.make_async_copy(cp_h, CP, ls.at[2]),
        pltpu.make_async_copy(wg_h, WC.at[:, pl.ds(0, CH)], ls.at[3]),
        pltpu.make_async_copy(wu_h, WC.at[:, pl.ds(CH, CH)], ls.at[4]),
        pltpu.make_async_copy(wd_h, WD, ls.at[5]),
        pltpu.make_async_copy(wo_h, WO, ls.at[6]),
    ]
    for load in loads:
        load.start()
    pl.semaphore_wait(barrier, 2 * (NS - 1))

    def active(t, d, h):
        return t <= 3 or d == h

    def ring(buf, index, half, ssem, rsem, t, d, h, arriving):
        sign = 1 - 2 * d
        block = buf.at[index(-sign * (t if arriving else t - 1)), pl.ds(h * half, half)]
        return remote(block, block, ssem.at[d, t - 1, h], rsem.at[d, t - 1, h], zdev(sign))

    def ring_send(*args):
        ring(*args, False).start()

    def ring_take(*args):
        ring(*args, True).wait_recv()

    def up_send(t):
        for d, h in STEPS:
            if active(t, d, h):
                ring_send(UP, zat, TOK // 2, ups, upr, t, d, h)

    def up_take(t):
        for d, h in STEPS:
            if active(t, d, h):
                ring_take(UP, zat, TOK // 2, ups, upr, t, d, h)

    loads[0].wait()
    up_send(1)

    def exchange_start(n, rows):
        SX[n] = rows
        SS[n, tp] = rows

        def step(k, carry):
            peer = (tp + k) % NS
            remote(SX.at[n], SS.at[n, tp], es.at[n], er.at[n], (sp, peer)).start()
            return carry

        lax.fori_loop(1, NS, step, 0)

    def exchange_end(n):
        many = SS.at[n, pl.ds(0, NS - 1)]
        remote(many, many, es.at[n], er.at[n], sibling).wait_recv()
        return rows_to_columns(jnp.sum(SS[n], axis=0))

    def exchange_flush(n):
        many = SS.at[n, pl.ds(0, NS - 1)]
        remote(many, many, es.at[n], er.at[n], sibling).wait_send()

    loads[1].wait()
    loads[2].wait()
    stream = ST[...].astype(F32)
    conv = CP[...].astype(F32)
    exchange_start(
        0,
        columns_to_rows([
            jnp.sum(stream * stream, axis=1, keepdims=True),
            jnp.sum(conv, axis=1, keepdims=True),
            jnp.sum(conv * conv, axis=1, keepdims=True),
        ]),
    )

    first, second = routes_ref[0:1, :], routes_ref[1:2, :]
    names = lax.broadcasted_iota(jnp.int32, (NS, TOK), 0)
    hit0 = (names == first).astype(F32)
    hit1 = (names == second).astype(F32)
    earlier = (
        lax.broadcasted_iota(jnp.int32, (TOK, TOK), 0) < lax.broadcasted_iota(jnp.int32, (TOK, TOK), 1)
    ).astype(F32).astype(BF16)
    rank = dot((hit0 + hit1).astype(BF16), earlier, 1, 0)
    slot0 = first * CAP + jnp.sum(hit0 * rank, axis=0, keepdims=True).astype(jnp.int32)
    slot1 = second * CAP + jnp.sum(hit1 * rank, axis=0, keepdims=True).astype(jnp.int32)
    for r in range(3):
        slots = lax.broadcasted_iota(jnp.int32, (TOK, TOK), 0) + r * TOK
        at0, at1 = slots == slot0, slots == slot1
        rows = pl.ds(r * TOK, TOK)
        PICK[rows, :] = jnp.logical_or(at0, at1).astype(F32).astype(BF16)
        SW[rows, :] = jnp.sum(
            jnp.where(at0, rw_ref[0:1, :], 0.0) + jnp.where(at1, rw_ref[1:2, :], 0.0),
            axis=1, keepdims=True,
        )

    def slot_rows(p):
        return pl.ds(pl.multiple_of(p * CAP, 16), CAP)

    def send_cotangent(offset):
        origin = zat(offset)
        block = mine(offset)

        def pick(r, carry):
            rows = pl.ds(pl.multiple_of(r * TOK, TOK), TOK)
            SC[origin, rows, :] = (dot(PICK[rows, :], UP[origin], 1, 0) * SW[rows, :]).astype(BF16)
            return carry

        lax.fori_loop(0, 3, pick, 0)

        def send(p):
            remote(
                SC.at[origin, slot_rows(p)], CT.at[block, slot_rows(sp)],
                cs.at[origin], cr.at[origin], (p, tp),
            ).start()

        each_peer(send)
        CT[block, slot_rows(sp), :] = SC[origin, slot_rows(sp), :]

    send_cotangent(0)
    up_take(1)
    up_send(2)

    stats = exchange_end(0)
    inverse = lax.rsqrt(stats[:, 0:1] / MODEL + EPSILON)
    mean_val = stats[:, 1:2] / CHANNELS
    inv_std = lax.rsqrt(stats[:, 2:3] / CHANNELS - mean_val * mean_val + EPSILON)
    normed = (gain_ref[...] * ST[...].astype(F32) * inverse).astype(BF16)
    for r in range(3):
        rows = pl.ds(r * TOK, TOK)
        SI[rows, :] = dot(PICK[rows, :], normed, 1, 0).astype(BF16)
    own = mine(0)

    def send_input(p):
        remote(SI.at[slot_rows(p)], X.at[own, slot_rows(sp)], as_.at[0], ar.at[0], (p, tp)).start()

    each_peer(send_input)
    X[own, slot_rows(sp), :] = SI[slot_rows(sp), :]

    send_cotangent(1)
    send_cotangent(-1)
    up_take(2)
    up_send(3)
    send_cotangent(2)
    send_cotangent(-2)
    up_take(3)
    up_send(4)
    send_cotangent(3)
    send_cotangent(-3)

    centred = (CP[...].astype(F32) - mean_val) * inv_std
    scaled = centred * lng_ref[...]
    CEN[...] = centred
    SCL[...] = scaled
    MO[...] = (scaled * jax.nn.sigmoid(scaled)).astype(BF16)
    G[...] = jnp.zeros_like(G)
    A[...] = jnp.zeros_like(A)

    up_take(4)
    send_cotangent(4)
    for k in range(3, 6):
        loads[k].wait()

    def take_many(dst, ssem, rsem):
        remote(dst, dst, ssem, rsem, sibling).wait_recv()

    def flush_many(src, ssem, rsem):
        remote(src, src, ssem, rsem, sibling).wait_send()

    def cols(j):
        return pl.ds(pl.multiple_of(j * W, W), W)

    def add_inputs(j):
        def step(r, carry):
            rows = pl.ds(pl.multiple_of(r * TOK, TOK), TOK)
            G[rows, :] = G[rows, :] + dot(X[j, rows, :], WC[cols(j), :], 1, 0)
            return carry

        lax.fori_loop(0, 3, step, 0)

    def add_cotangents(j):
        def step(r, carry):
            rows = pl.ds(pl.multiple_of(r * TOK, TOK), TOK)
            A[rows, :] = A[rows, :] + dot(CT[j, rows, :], WD[:, cols(j)], 1, 1)
            return carry

        lax.fori_loop(0, 3, step, 0)

    def hand_over(t, d, h, offset, arriving):
        j = other(offset) if arriving else mine(offset)
        block = X.at[j, pl.ds(h * HALF, HALF)]
        return remote(block, block, dxs.at[t, d, h], dxr.at[t, d, h], sibling)

    def x_ring(t, d, h):
        return (X, mine, HALF, xs, xr, t, d, h)

    def hand_cotangent(offset, arriving):
        j = other(offset) if arriving else mine(offset)
        return remote(CT.at[j], CT.at[j], dcs.at[zat(offset)], dcr.at[zat(offset)], sibling)

    take_many(X.at[own, pl.ds(0, ROWS - CAP)], as_.at[0], ar.at[0])
    for d, h in STEPS:
        ring_send(*x_ring(1, d, h))
    for h in range(2):
        hand_over(0, 0, h, 0, False).start()
    add_inputs(own)

    def stage_offsets(t):
        return (0,) if t == 0 else ((t, -t) if t < 4 else (4,))

    def x_chunks(t):
        if t == 0:
            return [(0, 0, 0), (0, 1, 0)]
        return [(d, h, -t * (1 - 2 * d)) for h in range(2) for d in range(2) if active(t, d, h)]

    def from_sibling(t):
        for d, h, offset in x_chunks(t):
            hand_over(t, d, h, offset, True).wait_recv()
        for offset in stage_offsets(t):
            add_inputs(other(offset))

    def cot_from_sibling(t):
        for offset in OFFSETS[2 * t - 2 : 2 * t]:
            hand_cotangent(offset, True).wait_recv()
            add_cotangents(other(offset))

    for t in range(1, 5):
        for d, h, offset in x_chunks(t):
            ring_take(*x_ring(t, d, h))
            if t < 4 and active(t + 1, d, h):
                ring_send(*x_ring(t + 1, d, h))
            hand_over(t, d, h, offset, False).start()
        for offset in stage_offsets(t):
            add_inputs(mine(offset))
        from_sibling(t - 1)
        for offset in OFFSETS[2 * t - 2 : 2 * t]:
            take_many(CT.at[mine(offset), pl.ds(0, ROWS - CAP)], cs.at[zat(offset)], cr.at[zat(offset)])
            hand_cotangent(offset, False).start()
            add_cotangents(mine(offset))
        if t > 1:
            cot_from_sibling(t - 1)
    from_sibling(4)
    cot_from_sibling(4)

    def hidden(r, carry):
        rows = pl.ds(pl.multiple_of(r * 64, 64), 64)
        gate, upper, back = G[rows, 0:CH], G[rows, CH : 2 * CH], A[rows, :]
        logistic = jax.nn.sigmoid(gate)
        silu = gate * logistic
        ACT[rows, :] = (silu * upper).astype(BF16)
        CAT[rows, 0:CH] = (back * upper * silu_slope(gate, logistic)).astype(BF16)
        CAT[rows, CH : 2 * CH] = (back * silu).astype(BF16)
        return carry

    lax.fori_loop(0, 12, hidden, 0)

    def sub_rows(h, r):
        return pl.ds(pl.multiple_of(h * HALF + r * 128, 128), 128)

    def for_sibling(offset):
        q = zat(offset)
        j = other(offset)

        def step(r, carry):
            rows = pl.ds(pl.multiple_of(r * TOK, TOK), TOK)
            SB[q, rows, :] = dot(CAT[rows, :], WC[cols(j), :], 1, 1).astype(BF16)
            return carry

        lax.fori_loop(0, 3, step, 0)
        remote(SB.at[q], SR.at[q], sbs.at[q], sbr.at[q], sibling).start()

    def take_sibling(offset):
        q = zat(offset)
        remote(SB.at[q], SR.at[q], sbs.at[q], sbr.at[q], sibling).wait_recv()

    def chip_part(offset, rows):
        return dot(CAT[rows, :], WC[cols(mine(offset)), :], 1, 1) + SR[zat(offset), rows, :].astype(F32)

    def rs_copy(d, k, h):
        part = pl.ds(h * HALF, HALF)
        return remote(
            RSS.at[d, k, part], RSR.at[d, k, part], rss.at[d, k, h], rsr.at[d, k, h], zdev(1 - 2 * d)
        )

    def rs_active(k, d, h):
        return k >= 1 or d == h

    def rs_send(k, d, h):
        offset = (4 - k) * (1 - 2 * d)
        incoming = k >= 1 and rs_active(k - 1, d, h)
        if incoming:
            rs_copy(d, k - 1, h).wait_recv()

        def step(r, carry):
            rows = sub_rows(h, r)
            total = chip_part(offset, rows)
            if incoming:
                total = total + RSR[d, k - 1, rows, :].astype(F32)
            RSS[d, k, rows, :] = total.astype(BF16)
            return carry

        lax.fori_loop(0, 3, step, 0)
        rs_copy(d, k, h).start()

    def gradients(first_block):
        def step(b, carry):
            j = first_block + b
            both = dot(X[j], CAT[...], 0, 0)
            GG[cols(j), :] = both[:, 0:CH]
            GU[cols(j), :] = both[:, CH : 2 * CH]
            GD[:, cols(j)] = dot(ACT[...], CT[j], 0, 0)
            return carry

        lax.fori_loop(0, 4, step, 0)

    for_sibling(4)
    for_sibling(3)
    for_sibling(-3)
    take_sibling(4)
    rs_send(0, 0, 0)
    rs_send(0, 1, 1)
    for_sibling(2)
    for_sibling(-2)
    take_sibling(3)
    take_sibling(-3)
    rs_send(1, 0, 1)
    rs_send(1, 1, 0)
    for_sibling(1)
    for_sibling(-1)
    for_sibling(0)
    rs_send(1, 0, 0)
    rs_send(1, 1, 1)
    gradients(0)
    take_sibling(2)
    take_sibling(-2)
    rs_send(2, 0, 1)
    rs_send(2, 1, 0)
    rs_send(2, 0, 0)
    rs_send(2, 1, 1)
    gradients(4)
    gradients(8)
    take_sibling(1)
    take_sibling(-1)
    rs_send(3, 0, 1)
    rs_send(3, 1, 0)
    rs_send(3, 0, 0)
    rs_send(3, 1, 1)
    gradients(12)
    stores = [
        pltpu.make_async_copy(GG, gg_h, ls.at[7]),
        pltpu.make_async_copy(GU, gu_h, ls.at[8]),
        pltpu.make_async_copy(GD, gd_h, ls.at[9]),
    ]
    for store in stores:
        store.start()
    take_sibling(0)
    for h in (1, 0):
        rs_copy(0, 3, h).wait_recv()
        rs_copy(1, 3, h).wait_recv()

        def finish(r, carry):
            rows = sub_rows(h, r)
            FIN[rows, :] = (
                chip_part(0, rows) + RSR[0, 3, rows, :].astype(F32) + RSR[1, 3, rows, :].astype(F32)
            ).astype(BF16)
            return carry

        lax.fori_loop(0, 3, finish, 0)

    def send_back(p):
        remote(FIN.at[slot_rows(p)], RET.at[slot_rows(sp)], fs.at[0], fr.at[0], (p, tp)).start()

    each_peer(send_back)
    RET[slot_rows(sp), :] = FIN[slot_rows(sp), :]
    take_many(RET.at[pl.ds(0, ROWS - CAP)], fs.at[0], fr.at[0])

    gained = gain_ref[...] * dot(PICK[...], RET[...], 0, 0)
    residual = ST[...].astype(F32)
    exchange_start(1, columns_to_rows([jnp.sum(gained * residual, axis=1, keepdims=True)]))
    inner = exchange_end(1)[:, 0:1] / MODEL
    SG[own] = (
        UP[z].astype(F32) + inverse * gained - residual * (inverse * inverse * inverse * inner)
    ).astype(BF16)

    def sg_ring(t, d, h):
        return (SG, mine, TOK // 2, sgs, sgr, t, d, h)

    def sg_hand(t, d, h, offset, arriving):
        j = other(offset) if arriving else mine(offset)
        block = SG.at[j, pl.ds(h * (TOK // 2), TOK // 2)]
        return remote(block, block, dgs.at[t, d, h], dgr.at[t, d, h], sibling)

    for d, h in STEPS:
        ring_send(*sg_ring(1, d, h))
    for h in range(2):
        sg_hand(0, 0, h, 0, False).start()
    loads[6].wait()

    def mix(j):
        MB[...] = MB[...] + dot(SG[j], WO[:, cols(j)], 1, 1)

    MB[...] = jnp.zeros_like(MB)
    mix(own)
    for t in range(1, 5):
        for d, h, offset in x_chunks(t):
            ring_take(*sg_ring(t, d, h))
            if t < 4 and active(t + 1, d, h):
                ring_send(*sg_ring(t + 1, d, h))
            sg_hand(t, d, h, offset, False).start()
        for offset in stage_offsets(t):
            mix(mine(offset))
        for d, h, offset in x_chunks(t - 1):
            sg_hand(t - 1, d, h, offset, True).wait_recv()
        for offset in stage_offsets(t - 1):
            mix(other(offset))
    for d, h, offset in x_chunks(4):
        sg_hand(4, d, h, offset, True).wait_recv()
    mix(other(4))

    scaled = SCL[...]
    norm_in = MB[...] * silu_slope(scaled, jax.nn.sigmoid(scaled)) * lng_ref[...]
    exchange_start(
        2,
        columns_to_rows([
            jnp.sum(norm_in, axis=1, keepdims=True),
            jnp.sum(norm_in * CEN[...], axis=1, keepdims=True),
        ]),
    )

    def out_block(p):
        GOS[p] = dot(MO[...], SG[p], 0, 0).astype(BF16)
        remote(GOS.at[p], GOR.at[sp], gs.at[0], gr.at[0], (p, tp)).start()

    def out_blocks(low, high):
        def step(k, carry):
            out_block((sp + k) % NS)
            return carry

        lax.fori_loop(low, high, step, 0)

    out_blocks(1, 6)
    sums = exchange_end(2)
    conv_back = inv_std * (
        norm_in - sums[:, 0:1] / CHANNELS - CEN[...] * (sums[:, 1:2] / CHANNELS)
    )
    HS[...] = conv_back[0:32, :]
    previous = ((sp + NS - 1) % NS, tp)

    @pl.when(sp > 0)
    def _():
        remote(HS, HALO, hs.at[0], hr.at[0], previous).start()

    cb_o[0:TOK, :] = conv_back
    out_blocks(6, NS)
    GOR[sp] = dot(MO[...], SG[sp], 0, 0).astype(BF16)

    @pl.when(sp < NS - 1)
    def _():
        remote(HS, HALO, hs.at[0], hr.at[0], previous).wait_recv()
        cb_o[TOK : TOK + 32, :] = HALO[...]

    @pl.when(sp == NS - 1)
    def _():
        cb_o[TOK : TOK + 32, :] = jnp.zeros((32, CH), F32)

    take_many(GOR.at[pl.ds(0, NS - 1)], gs.at[0], gr.at[0])

    def total(i, acc):
        return acc + GOR[i].astype(F32)

    go_o[...] = lax.fori_loop(0, NS, total, jnp.zeros((CH, W), F32))

    for t in range(1, 5):
        for d, h in STEPS:
            if active(t, d, h):
                ring(UP, zat, TOK // 2, ups, upr, t, d, h, False).wait_send()
                ring(*x_ring(t, d, h), False).wait_send()
                ring(*sg_ring(t, d, h), False).wait_send()
    for t in range(5):
        for d, h, offset in x_chunks(t):
            hand_over(t, d, h, offset, False).wait_send()
            sg_hand(t, d, h, offset, False).wait_send()
    for offset in OFFSETS:
        q = zat(offset)
        flush_many(SC.at[q, pl.ds(0, ROWS - CAP)], cs.at[q], cr.at[q])
        hand_cotangent(offset, False).wait_send()
        remote(SB.at[q], SR.at[q], sbs.at[q], sbr.at[q], sibling).wait_send()
    for k in range(4):
        for d, h in STEPS:
            if rs_active(k, d, h):
                rs_copy(d, k, h).wait_send()
    for n in range(3):
        exchange_flush(n)
    flush_many(SI.at[pl.ds(0, ROWS - CAP)], as_.at[0], ar.at[0])
    flush_many(FIN.at[pl.ds(0, ROWS - CAP)], fs.at[0], fr.at[0])
    flush_many(GOS.at[pl.ds(0, NS - 1)], gs.at[0], gr.at[0])

    @pl.when(sp > 0)
    def _():
        remote(HS, HALO, hs.at[0], hr.at[0], previous).wait_send()

    for store in stores:
        store.wait()


def last_kernel(
    gg_i, gu_i, gd_i, cb_ref, taps_ref, value_ref, gate_ref,
    gg_o, gu_o, gd_o, vg_o, tg_o, bufs_tall, buf_wide, lsem, ssem,
):
    pieces = []
    for a, (src, dst) in enumerate(((gg_i, gg_o), (gu_i, gu_o))):
        for q in range(4):
            part = pl.ds(q * 1024, 1024)
            pieces.append((src.at[part], bufs_tall.at[a, part], dst.at[part]))
    for q in range(4):
        part = pl.ds(q * 32, 32)
        pieces.append((gd_i.at[part], buf_wide.at[part], gd_o.at[part]))
    ins = [pltpu.make_async_copy(s, b, lsem.at[n]) for n, (s, b, _) in enumerate(pieces)]
    outs = [pltpu.make_async_copy(b, d, ssem.at[n]) for n, (_, b, d) in enumerate(pieces)]
    for copy in ins:
        copy.start()
    for i, o in zip(ins, outs):
        i.wait()
        o.start()
    acc = jnp.zeros((TOK, CH), F32)
    for tap in range(TAPS):
        acc = acc + taps_ref[tap : tap + 1, :] * cb_ref[TAPS - 1 - tap : TAPS - 1 - tap + TOK, :]
    sigma = jax.nn.sigmoid(gate_ref[...].astype(F32))
    vg_o[...] = (acc * sigma).astype(BF16)
    tg_o[...] = (acc * value_ref[...].astype(F32) * sigma * (1.0 - sigma)).astype(BF16)
    for copy in outs:
        copy.wait()


def shape(dims, dtype):
    return jax.ShapeDtypeStruct(dims, dtype)


def per_device(
    upstream, stream, norm_gain, routes, route_weights, w_gate, w_up, w_down,
    value_in, gate_in, conv_pre, ln_gain, conv_taps, w_out,
):
    near, far = pl.BlockSpec(memory_space=pltpu.VMEM), pl.BlockSpec(memory_space=pl.ANY)
    dma, vm = pltpu.SemaphoreType.DMA, pltpu.VMEM
    grads = [shape((MODEL, CH), F32), shape((MODEL, CH), F32), shape((CH, MODEL), F32)]
    scratch = [
        vm((NZ, TOK, W), BF16), vm((TOK, W), BF16), vm((TOK, CH), BF16),
        vm((MODEL, 2 * CH), BF16), vm((CH, MODEL), BF16), vm((CH, MODEL), BF16),
        vm((ROWS, TOK), BF16), vm((ROWS, 1), F32),
        vm((ROWS, W), BF16), vm((NZ, ROWS, W), BF16),
        vm((NS, ROWS, W), BF16), vm((NS, ROWS, W), BF16),
        vm((ROWS, 2 * CH), F32), vm((ROWS, CH), F32),
        vm((ROWS, 2 * CH), BF16), vm((ROWS, CH), BF16),
        vm((MODEL, CH), F32), vm((MODEL, CH), F32), vm((CH, MODEL), F32),
        vm((NZ, ROWS, W), BF16), vm((NZ, ROWS, W), BF16),
        vm((2, 4, ROWS, W), BF16), vm((2, 4, ROWS, W), BF16),
        vm((ROWS, W), BF16), vm((ROWS, W), BF16),
        vm((NS, TOK, W), BF16), vm((TOK, CH), F32),
        vm((TOK, CH), BF16), vm((TOK, CH), F32), vm((TOK, CH), F32),
        vm((32, CH), F32), vm((32, CH), F32),
        vm((NS, CH, W), BF16), vm((NS, CH, W), BF16),
        vm((3, NS, 8, TOK), F32), vm((3, 8, TOK), F32),
        dma((10,)),
        dma((2, 4, 2)), dma((2, 4, 2)), dma((2, 4, 2)), dma((2, 4, 2)),
        dma((5, 2, 2)), dma((5, 2, 2)),
        dma((1,)), dma((1,)),
        dma((NZ,)), dma((NZ,)), dma((NZ,)), dma((NZ,)),
        dma((NZ,)), dma((NZ,)),
        dma((2, 4, 2)), dma((2, 4, 2)),
        dma((3,)), dma((3,)),
        dma((1,)), dma((1,)),
        dma((2, 4, 2)), dma((2, 4, 2)), dma((5, 2, 2)), dma((5, 2, 2)),
        dma((1,)), dma((1,)), dma((1,)), dma((1,)),
    ]
    gg, gu, gd, conv_back, grad_out = pl.pallas_call(
        comm_kernel,
        name="exchange",
        out_shape=grads + [shape((TOK + 32, CH), F32), shape((CH, W), F32)],
        in_specs=[near] * 4 + [far] * 7,
        out_specs=[far] * 3 + [near] * 2,
        scratch_shapes=scratch,
        compiler_params=pltpu.CompilerParams(
            collective_id=0, has_side_effects=True, vmem_limit_bytes=67_000_000
        ),
    )(
        norm_gain.reshape(1, W), routes.T, route_weights.T, ln_gain.reshape(1, CH),
        upstream, stream, w_gate[0], w_up[0], w_down[0], conv_pre, w_out,
    )
    grad_gate, grad_up, grad_down, value_grad, gate_grad = pl.pallas_call(
        last_kernel,
        name="last",
        out_shape=grads + [shape((TOK, CH), BF16)] * 2,
        in_specs=[far] * 3 + [near] * 4,
        out_specs=[far] * 3 + [near] * 2,
        scratch_shapes=[
            vm((2, MODEL, CH), F32), vm((CH, MODEL), F32), dma((12,)), dma((12,)),
        ],
        compiler_params=pltpu.CompilerParams(vmem_limit_bytes=40_000_000),
    )(gg, gu, gd, conv_back, conv_taps, value_in, gate_in)
    return (grad_gate[None], grad_up[None], grad_down[None], grad_out, value_grad, gate_grad)


def solution(mesh):
    return jax.shard_map(
        per_device,
        mesh=mesh,
        in_specs=(
            P("sp", "tp"), P("sp", "tp"), P("tp"), P("sp", None), P("sp", None),
            P("sp", None, "tp"), P("sp", None, "tp"), P("sp", "tp", None),
            P("sp", "tp"), P("sp", "tp"), P("sp", "tp"), P("tp"), P(None, "tp"), P("tp", None),
        ),
        out_specs=(
            P("sp", None, "tp"), P("sp", None, "tp"), P("sp", "tp", None),
            P("tp", "sp"), P("sp", "tp"), P("sp", "tp"),
        ),
        check_vma=False,
    )
```

```python
import jax
import jax.numpy as jnp
from jax import lax
from jax.experimental import pallas as pl
from jax.experimental.pallas import tpu as pltpu
from jax.sharding import PartitionSpec as P

MESH = pl.DeviceIdType.MESH
F32, BF16 = jnp.float32, jnp.bfloat16
EPSILON = 1e-06
NZ, NS = 8, 16
TOK, W, CH = 256, 256, 128
CAP, ROWS, HALF = 48, 768, 384
MODEL, CHANNELS, TAPS = 4096, 2048, 31
STEPS = ((0, 0), (0, 1), (1, 0), (1, 1))
OFFSETS = (0, 1, -1, 2, -2, 3, -3, 4)


def dot(a, b, ca, cb):
    return lax.dot_general(a, b, (((ca,), (cb,)), ((), ())), preferred_element_type=F32)


def columns_to_rows(columns):
    lane = lax.broadcasted_iota(jnp.int32, (TOK, 128), 1)
    packed = jnp.zeros((TOK, 128), F32)
    for k, column in enumerate(columns):
        packed = jnp.where(lane == k, column, packed)
    return packed.T[0:8, :]


def rows_to_columns(rows):
    return jnp.concatenate([rows, jnp.zeros((120, TOK), F32)], axis=0).T


def silu_slope(values, logistic):
    return logistic * (1.0 + values * (1.0 - logistic))


def comm_kernel(
    gain_ref, routes_ref, rw_ref, lng_ref, up_h, st_h, wg_h, wu_h, wd_h, cp_h, wo_h,
    gg_h, gu_h, gd_h, cb_o, go_o,
    UP, XS, CP, WC, WD, WO, PICK, SW, SI, SC, X, CT, G, A, CAT, ACT, GG, GU, GD,
    SB, SR, RSS, RSR, PB, RB, TSS, TSR, TB, AP, FIN, RET, SG, MB, MO, CEN, SCL, HS, HALO, GOS, GOR, SS, SX,
    ls, ups, upr, xs, xr, dxs, dxr, as_, ar, cs, cr, dcs, dcr, sbs, sbr, rss, rsr, bs, br, tss, tsr,
    sts, str_, dts, dtr, es, er, fs, fr, sgs, sgr, dgs, dgr, gs, gr, hs, hr,
):
    sp = lax.axis_index("sp")
    tp = lax.axis_index("tp")
    z = tp // 2
    c = tp % 2
    sibling = (sp, z * 2 + 1 - c)

    def zat(offset):
        return (z + offset + NZ) % NZ

    def zdev(offset):
        return (sp, zat(offset) * 2 + c)

    def mine(offset):
        return zat(offset) * 2 + c

    def other(offset):
        return zat(offset) * 2 + 1 - c

    def remote(src, dst, ssem, rsem, device):
        return pltpu.make_async_remote_copy(
            src_ref=src, dst_ref=dst, send_sem=ssem, recv_sem=rsem,
            device_id=device, device_id_type=MESH,
        )

    def each_peer(body):
        def step(k, carry):
            body((sp + k) % NS)
            return carry

        lax.fori_loop(1, NS, step, 0)

    barrier = pltpu.get_barrier_semaphore()

    def greet(k, carry):
        pl.semaphore_signal(barrier, inc=1, device_id=(sp, (tp + k) % NS), device_id_type=MESH)
        pl.semaphore_signal(barrier, inc=1, device_id=((sp + k) % NS, tp), device_id_type=MESH)
        return carry

    lax.fori_loop(1, NS, greet, 0)
    loads = [
        pltpu.make_async_copy(up_h, UP.at[z], ls.at[0]),
        pltpu.make_async_copy(st_h, XS.at[mine(0)], ls.at[1]),
        pltpu.make_async_copy(cp_h, CP, ls.at[2]),
        pltpu.make_async_copy(wg_h, WC.at[:, pl.ds(0, CH)], ls.at[3]),
        pltpu.make_async_copy(wu_h, WC.at[:, pl.ds(CH, CH)], ls.at[4]),
        pltpu.make_async_copy(wd_h, WD, ls.at[5]),
        pltpu.make_async_copy(wo_h, WO, ls.at[6]),
    ]
    for load in loads:
        load.start()

    def active(t, d, h):
        return t <= 3 or d == h

    def ring(buf, index, half, ssem, rsem, t, d, h, arriving):
        sign = 1 - 2 * d
        block = buf.at[index(-sign * (t if arriving else t - 1)), pl.ds(h * half, half)]
        return remote(block, block, ssem.at[d, t - 1, h], rsem.at[d, t - 1, h], zdev(sign))

    def ring_send(*args):
        ring(*args, False).start()

    def ring_take(*args):
        ring(*args, True).wait_recv()

    def halves_ring(buf, ssem, rsem):
        def send(t):
            for h in range(2):
                for d in range(2):
                    if active(t, d, h):
                        ring_send(buf, mine, TOK // 2, ssem, rsem, t, d, h)

        def hand(t, d, h, offset, arriving, hs_, hr_):
            j = other(offset) if arriving else mine(offset)
            block = buf.at[j, pl.ds(h * (TOK // 2), TOK // 2)]
            return remote(block, block, hs_.at[t, d, h], hr_.at[t, d, h], sibling)

        return send, hand

    def x_chunks(t):
        if t == 0:
            return [(0, 0, 0), (0, 1, 0)]
        return [(d, h, -t * (1 - 2 * d)) for h in range(2) for d in range(2) if active(t, d, h)]

    xs_send, xs_hand_ = halves_ring(XS, sts, str_)

    def xs_hand(t, d, h, offset, arriving):
        return xs_hand_(t, d, h, offset, arriving, dts, dtr)

    def xs_take(t):
        for d, h, offset in x_chunks(t):
            ring_take(XS, mine, TOK // 2, sts, str_, t, d, h)
            if t < 4 and active(t + 1, d, h):
                ring_send(XS, mine, TOK // 2, sts, str_, t + 1, d, h)
            xs_hand(t, d, h, offset, False).start()

    def up_take(t):
        for h in range(2):
            for d in range(2):
                if active(t, d, h):
                    ring_take(UP, zat, TOK // 2, ups, upr, t, d, h)
                    if t < 4 and active(t + 1, d, h):
                        ring_send(UP, zat, TOK // 2, ups, upr, t + 1, d, h)

    def exchange_set(n, rows):
        SX[n] = rows
        SS[n, tp] = rows

    def exchange_start(n):
        def step(k, carry):
            peer = (tp + k) % NS
            remote(SX.at[n], SS.at[n, tp], es.at[n], er.at[n], (sp, peer)).start()
            return carry

        lax.fori_loop(1, NS, step, 0)

    def exchange_end(n):
        many = SS.at[n, pl.ds(0, NS - 1)]
        remote(many, many, es.at[n], er.at[n], sibling).wait_recv()
        return rows_to_columns(jnp.sum(SS[n], axis=0))

    def exchange_flush(n):
        many = SS.at[n, pl.ds(0, NS - 1)]
        remote(many, many, es.at[n], er.at[n], sibling).wait_send()

    loads[1].wait()
    loads[2].wait()
    stream = XS[mine(0)].astype(F32)
    conv = CP[...].astype(F32)
    exchange_set(
        0,
        columns_to_rows([
            jnp.sum(stream * stream, axis=1, keepdims=True),
            jnp.sum(conv, axis=1, keepdims=True),
            jnp.sum(conv * conv, axis=1, keepdims=True),
        ]),
    )

    first, second = routes_ref[0:1, :], routes_ref[1:2, :]
    names = lax.broadcasted_iota(jnp.int32, (NS, TOK), 0)
    hit0 = (names == first).astype(F32)
    hit1 = (names == second).astype(F32)
    earlier = (
        lax.broadcasted_iota(jnp.int32, (TOK, TOK), 0) < lax.broadcasted_iota(jnp.int32, (TOK, TOK), 1)
    ).astype(F32).astype(BF16)
    rank = dot((hit0 + hit1).astype(BF16), earlier, 1, 0)
    slot0 = first * CAP + jnp.sum(hit0 * rank, axis=0, keepdims=True).astype(jnp.int32)
    slot1 = second * CAP + jnp.sum(hit1 * rank, axis=0, keepdims=True).astype(jnp.int32)
    for r in range(3):
        slots = lax.broadcasted_iota(jnp.int32, (TOK, TOK), 0) + r * TOK
        at0, at1 = slots == slot0, slots == slot1
        rows = pl.ds(r * TOK, TOK)
        PICK[rows, :] = jnp.logical_or(at0, at1).astype(F32).astype(BF16)
        SW[rows, :] = jnp.sum(
            jnp.where(at0, rw_ref[0:1, :], 0.0) + jnp.where(at1, rw_ref[1:2, :], 0.0),
            axis=1, keepdims=True,
        )

    def slot_rows(p):
        return pl.ds(pl.multiple_of(p * CAP, 16), CAP)

    def pick_cotangent(offset):
        origin = zat(offset)

        def pick(r, carry):
            rows = pl.ds(pl.multiple_of(r * TOK, TOK), TOK)
            SC[origin, rows, :] = (dot(PICK[rows, :], UP[origin], 1, 0) * SW[rows, :]).astype(BF16)
            return carry

        lax.fori_loop(0, 3, pick, 0)

    def send_cotangent(offset):
        origin = zat(offset)
        block = mine(offset)

        def send(p):
            remote(
                SC.at[origin, slot_rows(p)], CT.at[block, slot_rows(sp)],
                cs.at[origin], cr.at[origin], (p, tp),
            ).start()

        each_peer(send)
        CT[block, slot_rows(sp), :] = SC[origin, slot_rows(sp), :]

    def cotangent(offset):
        pick_cotangent(offset)
        send_cotangent(offset)

    loads[0].wait()
    pick_cotangent(0)
    pl.semaphore_wait(barrier, 2 * (NS - 1))
    exchange_start(0)
    for h in range(2):
        for d in range(2):
            ring_send(UP, zat, TOK // 2, ups, upr, 1, d, h)
    send_cotangent(0)
    up_take(1)
    stats = exchange_end(0)
    inverse = lax.rsqrt(stats[:, 0:1] / MODEL + EPSILON)
    mean_val = stats[:, 1:2] / CHANNELS
    inv_std = lax.rsqrt(stats[:, 2:3] / CHANNELS - mean_val * mean_val + EPSILON)
    normed = (gain_ref[...] * XS[mine(0)].astype(F32) * inverse).astype(BF16)
    for r in range(3):
        rows = pl.ds(r * TOK, TOK)
        SI[rows, :] = dot(PICK[rows, :], normed, 1, 0).astype(BF16)
    own = mine(0)

    def send_input(p):
        remote(SI.at[slot_rows(p)], X.at[own, slot_rows(sp)], as_.at[0], ar.at[0], (p, tp)).start()

    each_peer(send_input)
    X[own, slot_rows(sp), :] = SI[slot_rows(sp), :]

    cotangent(1)
    cotangent(-1)
    up_take(2)
    centred = (CP[...].astype(F32) - mean_val) * inv_std
    scaled = centred * lng_ref[...]
    CEN[...] = centred
    SCL[...] = scaled
    MO[...] = (scaled * jax.nn.sigmoid(scaled)).T.astype(BF16)
    G[...] = jnp.zeros_like(G)
    A[...] = jnp.zeros_like(A)

    for k in range(3, 6):
        loads[k].wait()

    def take_many(dst, ssem, rsem):
        remote(dst, dst, ssem, rsem, sibling).wait_recv()

    def flush_many(src, ssem, rsem):
        remote(src, src, ssem, rsem, sibling).wait_send()

    def cols(j):
        return pl.ds(pl.multiple_of(j * W, W), W)

    def add_inputs(blocks):
        total = G[...]
        for j in blocks:
            total = total + dot(X[j], WC[cols(j), :], 1, 0)
        G[...] = total

    def add_cotangents(blocks):
        total = A[...]
        for j in blocks:
            total = total + dot(CT[j], WD[:, cols(j)], 1, 1)
        A[...] = total

    def hand_over(t, d, h, offset, arriving):
        j = other(offset) if arriving else mine(offset)
        block = X.at[j, pl.ds(h * HALF, HALF)]
        return remote(block, block, dxs.at[t, d, h], dxr.at[t, d, h], sibling)

    def x_ring(t, d, h):
        return (X, mine, HALF, xs, xr, t, d, h)

    def hand_cotangent(offset, arriving):
        j = other(offset) if arriving else mine(offset)
        return remote(CT.at[j], CT.at[j], dcs.at[zat(offset)], dcr.at[zat(offset)], sibling)

    take_many(X.at[own, pl.ds(0, ROWS - CAP)], as_.at[0], ar.at[0])
    for d, h in STEPS:
        ring_send(*x_ring(1, d, h))
    for h in range(2):
        hand_over(0, 0, h, 0, False).start()
    add_inputs([own])
    cotangent(2)
    cotangent(-2)
    up_take(3)
    cotangent(3)
    cotangent(-3)

    def stage_offsets(t):
        return (0,) if t == 0 else ((t, -t) if t < 4 else (4,))

    def from_sibling(t):
        for d, h, offset in x_chunks(t):
            hand_over(t, d, h, offset, True).wait_recv()
        add_inputs([other(offset) for offset in stage_offsets(t)])

    def cot_own(offsets):
        for offset in offsets:
            take_many(CT.at[mine(offset), pl.ds(0, ROWS - CAP)], cs.at[zat(offset)], cr.at[zat(offset)])
            hand_cotangent(offset, False).start()
        add_cotangents([mine(offset) for offset in offsets])

    def cot_other(offsets):
        for offset in offsets:
            hand_cotangent(offset, True).wait_recv()
        add_cotangents([other(offset) for offset in offsets])

    cot_stages = ((0, 1), (-1, 2, -2), (3, -3), (4,))
    for t in range(1, 5):
        for d, h, offset in x_chunks(t):
            ring_take(*x_ring(t, d, h))
            if t < 4 and active(t + 1, d, h):
                ring_send(*x_ring(t + 1, d, h))
            hand_over(t, d, h, offset, False).start()
        if t == 1:
            up_take(4)
            cotangent(4)
        if t == 3:
            xs_send(1)
            for h in range(2):
                xs_hand(0, 0, h, 0, False).start()
        if t == 4:
            xs_take(1)
        add_inputs([mine(offset) for offset in stage_offsets(t)])
        from_sibling(t - 1)
        cot_own(cot_stages[t - 1])
        if t > 1:
            cot_other(cot_stages[t - 2])
    from_sibling(4)
    cot_other(cot_stages[3])

    def hidden(r, carry):
        rows = pl.ds(pl.multiple_of(r * 64, 64), 64)
        gate, upper, back = G[rows, 0:CH], G[rows, CH : 2 * CH], A[rows, :]
        logistic = jax.nn.sigmoid(gate)
        silu = gate * logistic
        ACT[rows, :] = (silu * upper).astype(BF16)
        CAT[rows, 0:CH] = (back * upper * silu_slope(gate, logistic)).astype(BF16)
        CAT[rows, CH : 2 * CH] = (back * silu).astype(BF16)
        return carry

    lax.fori_loop(0, 12, hidden, 0)

    def for_sibling(offset):
        q = zat(offset)
        j = other(offset)

        SB[q] = dot(CAT[...], WC[cols(j), :], 1, 1).astype(BF16)
        remote(SB.at[q], SR.at[q], sbs.at[q], sbr.at[q], sibling).start()

    def take_sibling(offset):
        q = zat(offset)
        remote(SB.at[q], SR.at[q], sbs.at[q], sbr.at[q], sibling).wait_recv()

    def chip_part(offset):
        q = zat(offset)
        take_sibling(offset)
        part = dot(CAT[...], WC[cols(mine(offset)), :], 1, 1) + SR[q].astype(F32)
        AP[q] = part[:, 0:CH]
        PB[q] = part[:, CH : 2 * CH].astype(BF16)

        def send(p):
            remote(PB.at[q, slot_rows(p)], RB.at[q, slot_rows(sp)], bs.at[q], br.at[q], (p, tp)).start()

        each_peer(send)
        RB[q, slot_rows(sp), :] = PB[q, slot_rows(sp), :]

    def rs_copy(d, k, h):
        part = pl.ds(h * HALF, HALF)
        return remote(
            RSS.at[d, k, part], RSR.at[d, k, part], rss.at[d, k, h], rsr.at[d, k, h], zdev(1 - 2 * d)
        )

    def rs_active(k, d, h):
        return k >= 1 or d == h

    def rs_send(k, d, h):
        offset = (4 - k) * (1 - 2 * d)
        incoming = k >= 1 and rs_active(k - 1, d, h)
        if incoming:
            rs_copy(d, k - 1, h).wait_recv()

        part = slice(h * HALF, h * HALF + HALF)
        total = AP[zat(offset), part, :]
        if incoming:
            total = total + RSR[d, k - 1, part, :].astype(F32)
        RSS[d, k, part, :] = total.astype(BF16)
        rs_copy(d, k, h).start()

    def back_take(offset):
        q = zat(offset)
        take_many(RB.at[q, pl.ds(0, ROWS - CAP)], bs.at[q], br.at[q])

    def token_part(offset, h):
        return dot(PICK[:, h * CH : h * CH + CH], RB[zat(offset)], 0, 0)

    def ts_copy(d, k, h):
        part = pl.ds(h * CH, CH)
        return remote(
            TSS.at[d, k, part], TSR.at[d, k, part], tss.at[d, k, h], tsr.at[d, k, h], zdev(1 - 2 * d)
        )

    def ts_send(k, d, h):
        total = token_part((4 - k) * (1 - 2 * d), h)
        if k >= 1 and rs_active(k - 1, d, h):
            ts_copy(d, k - 1, h).wait_recv()
            total = total + TSR[d, k - 1, h * CH : h * CH + CH, :].astype(F32)
        TSS[d, k, h * CH : h * CH + CH, :] = total.astype(BF16)
        ts_copy(d, k, h).start()

    def ts_step(k):
        for offset in stage_offsets(4 - k):
            back_take(offset)
        for d, h in ((0, 1), (1, 0), (0, 0), (1, 1)):
            if rs_active(k, d, h):
                ts_send(k, d, h)

    def rs_step(k):
        for d, h in ((0, 1), (1, 0), (0, 0), (1, 1)):
            if rs_active(k, d, h):
                rs_send(k, d, h)

    def gradients(first_block):
        def step(b, carry):
            j = first_block + b
            both = dot(X[j], CAT[...], 0, 0)
            GG[cols(j), :] = both[:, 0:CH]
            GU[cols(j), :] = both[:, CH : 2 * CH]
            GD[:, cols(j)] = dot(ACT[...], CT[j], 0, 0)
            return carry

        lax.fori_loop(0, 4, step, 0)

    for_sibling(4)
    for_sibling(3)
    for_sibling(-3)
    xs_take(2)
    chip_part(4)
    rs_step(0)
    chip_part(3)
    chip_part(-3)
    for_sibling(2)
    for_sibling(-2)
    xs_take(3)
    rs_step(1)
    chip_part(2)
    chip_part(-2)
    for_sibling(1)
    for_sibling(-1)
    for_sibling(0)
    rs_step(2)
    chip_part(1)
    chip_part(-1)
    chip_part(0)
    ts_step(0)
    xs_take(4)
    gradients(0)
    rs_step(3)
    ts_step(1)
    gradients(4)
    ts_step(2)
    for h in range(2):
        rs_copy(0, 3, h).wait_recv()
        rs_copy(1, 3, h).wait_recv()

        part = slice(h * HALF, h * HALF + HALF)
        FIN[part, :] = (
            AP[z, part, :] + RSR[0, 3, part, :].astype(F32) + RSR[1, 3, part, :].astype(F32)
        ).astype(BF16)

    def send_back(p):
        remote(FIN.at[slot_rows(p)], RET.at[slot_rows(sp)], fs.at[0], fr.at[0], (p, tp)).start()

    each_peer(send_back)
    RET[slot_rows(sp), :] = FIN[slot_rows(sp), :]
    gradients(8)
    ts_step(3)
    gradients(12)
    stores = [
        pltpu.make_async_copy(GG, gg_h, ls.at[7]),
        pltpu.make_async_copy(GU, gu_h, ls.at[8]),
        pltpu.make_async_copy(GD, gd_h, ls.at[9]),
    ]
    for store in stores:
        store.start()
    back_take(0)
    for h in range(2):
        part = slice(h * CH, h * CH + CH)
        total = token_part(0, h)
        for d in range(2):
            ts_copy(d, 3, h).wait_recv()
            total = total + TSR[d, 3, part, :].astype(F32)
        TB[part, CH : 2 * CH] = total
    take_many(RET.at[pl.ds(0, ROWS - CAP)], fs.at[0], fr.at[0])
    TB[:, 0:CH] = dot(PICK[...], RET[...], 0, 0)

    gained = gain_ref[...] * TB[...]
    residual = XS[mine(0)].astype(F32)
    exchange_set(1, columns_to_rows([jnp.sum(gained * residual, axis=1, keepdims=True)]))
    exchange_start(1)
    SG[own] = (UP[z].astype(F32) + inverse * gained).astype(BF16)

    def sg_ring(t, d, h):
        return (SG, mine, TOK // 2, sgs, sgr, t, d, h)

    def sg_hand(t, d, h, offset, arriving):
        j = other(offset) if arriving else mine(offset)
        block = SG.at[j, pl.ds(h * (TOK // 2), TOK // 2)]
        return remote(block, block, dgs.at[t, d, h], dgr.at[t, d, h], sibling)

    for d, h in STEPS:
        ring_send(*sg_ring(1, d, h))
    for h in range(2):
        sg_hand(0, 0, h, 0, False).start()
    loads[6].wait()

    def mix(j):
        block = (SG[j].astype(F32) - XS[j].astype(F32) * share).astype(BF16)
        part = dot(MO[...], block, 1, 0).astype(BF16)

        @pl.when(j == sp)
        def _():
            GOR[sp] = part

        @pl.when(j != sp)
        def _():
            GOS[j] = part
            remote(GOS.at[j], GOR.at[sp], gs.at[0], gr.at[0], (j, tp)).start()

        MB[...] = MB[...] + dot(block, WO[:, cols(j)], 1, 1)

    MB[...] = jnp.zeros_like(MB)

    def mix_other(t):
        for d, h, offset in x_chunks(t):
            xs_hand(t, d, h, offset, True).wait_recv()
            sg_hand(t, d, h, offset, True).wait_recv()
        for offset in stage_offsets(t):
            mix(other(offset))

    for t in range(1, 5):
        for d, h, offset in x_chunks(t):
            ring_take(*sg_ring(t, d, h))
            if t < 4 and active(t + 1, d, h):
                ring_send(*sg_ring(t + 1, d, h))
            sg_hand(t, d, h, offset, False).start()
        if t == 1:
            inner = exchange_end(1)[:, 0:1] / MODEL
            share = inverse * inverse * inverse * inner
            mix(own)
        for offset in stage_offsets(t):
            mix(mine(offset))
        mix_other(t - 1)
    mix_other(4)

    scaled = SCL[...]
    norm_in = MB[...] * silu_slope(scaled, jax.nn.sigmoid(scaled)) * lng_ref[...]
    exchange_set(
        2,
        columns_to_rows([
            jnp.sum(norm_in, axis=1, keepdims=True),
            jnp.sum(norm_in * CEN[...], axis=1, keepdims=True),
        ]),
    )
    exchange_start(2)

    sums = exchange_end(2)
    conv_back = inv_std * (
        norm_in - sums[:, 0:1] / CHANNELS - CEN[...] * (sums[:, 1:2] / CHANNELS)
    )
    HS[...] = conv_back[0:32, :]
    previous = ((sp + NS - 1) % NS, tp)

    @pl.when(sp > 0)
    def _():
        remote(HS, HALO, hs.at[0], hr.at[0], previous).start()

    cb_o[0:TOK, :] = conv_back

    @pl.when(sp < NS - 1)
    def _():
        remote(HS, HALO, hs.at[0], hr.at[0], previous).wait_recv()
        cb_o[TOK : TOK + 32, :] = HALO[...]

    @pl.when(sp == NS - 1)
    def _():
        cb_o[TOK : TOK + 32, :] = jnp.zeros((32, CH), F32)

    take_many(GOR.at[pl.ds(0, NS - 1)], gs.at[0], gr.at[0])

    def total(i, acc):
        return acc + GOR[i].astype(F32)

    go_o[...] = lax.fori_loop(0, NS, total, jnp.zeros((CH, W), F32))

    for t in range(1, 5):
        for d, h in STEPS:
            if active(t, d, h):
                ring(UP, zat, TOK // 2, ups, upr, t, d, h, False).wait_send()
                ring(*x_ring(t, d, h), False).wait_send()
                ring(*sg_ring(t, d, h), False).wait_send()
                ring(XS, mine, TOK // 2, sts, str_, t, d, h, False).wait_send()
    for t in range(5):
        for d, h, offset in x_chunks(t):
            hand_over(t, d, h, offset, False).wait_send()
            sg_hand(t, d, h, offset, False).wait_send()
            xs_hand(t, d, h, offset, False).wait_send()
    for offset in OFFSETS:
        q = zat(offset)
        flush_many(SC.at[q, pl.ds(0, ROWS - CAP)], cs.at[q], cr.at[q])
        hand_cotangent(offset, False).wait_send()
        flush_many(PB.at[q, pl.ds(0, ROWS - CAP)], bs.at[q], br.at[q])
        remote(SB.at[q], SR.at[q], sbs.at[q], sbr.at[q], sibling).wait_send()
    for k in range(4):
        for d, h in STEPS:
            if rs_active(k, d, h):
                rs_copy(d, k, h).wait_send()
                ts_copy(d, k, h).wait_send()
    for n in range(3):
        exchange_flush(n)
    flush_many(SI.at[pl.ds(0, ROWS - CAP)], as_.at[0], ar.at[0])
    flush_many(FIN.at[pl.ds(0, ROWS - CAP)], fs.at[0], fr.at[0])
    flush_many(GOS.at[pl.ds(0, NS - 1)], gs.at[0], gr.at[0])

    @pl.when(sp > 0)
    def _():
        remote(HS, HALO, hs.at[0], hr.at[0], previous).wait_send()

    for store in stores:
        store.wait()


def last_kernel(
    gg_i, gu_i, gd_i, cb_ref, go_ref, taps_ref, value_ref, gate_ref,
    gg_o, gu_o, gd_o, vg_o, tg_o, go_o, bufs_tall, buf_wide, lsem, ssem,
):
    pieces = []
    for a, (src, dst) in enumerate(((gg_i, gg_o), (gu_i, gu_o))):
        for q in range(4):
            part = pl.ds(q * 1024, 1024)
            pieces.append((src.at[part], bufs_tall.at[a, part], dst.at[part]))
    for q in range(4):
        part = pl.ds(q * 32, 32)
        pieces.append((gd_i.at[part], buf_wide.at[part], gd_o.at[part]))
    ins = [pltpu.make_async_copy(s, b, lsem.at[n]) for n, (s, b, _) in enumerate(pieces)]
    outs = [pltpu.make_async_copy(b, d, ssem.at[n]) for n, (_, b, d) in enumerate(pieces)]
    for copy in ins:
        copy.start()
    for i, o in zip(ins, outs):
        i.wait()
        o.start()
    go_o[...] = go_ref[...]
    acc = jnp.zeros((TOK, CH), F32)
    for tap in range(TAPS):
        acc = acc + taps_ref[tap : tap + 1, :] * cb_ref[TAPS - 1 - tap : TAPS - 1 - tap + TOK, :]
    sigma = jax.nn.sigmoid(gate_ref[...].astype(F32))
    vg_o[...] = (acc * sigma).astype(BF16)
    tg_o[...] = (acc * value_ref[...].astype(F32) * sigma * (1.0 - sigma)).astype(BF16)
    for copy in outs:
        copy.wait()


def shape(dims, dtype):
    return jax.ShapeDtypeStruct(dims, dtype)


def per_device(
    upstream, stream, norm_gain, routes, route_weights, w_gate, w_up, w_down,
    value_in, gate_in, conv_pre, ln_gain, conv_taps, w_out,
):
    near, far = pl.BlockSpec(memory_space=pltpu.VMEM), pl.BlockSpec(memory_space=pl.ANY)
    dma, vm = pltpu.SemaphoreType.DMA, pltpu.VMEM
    grads = [shape((MODEL, CH), F32), shape((MODEL, CH), F32), shape((CH, MODEL), F32)]
    scratch = [
        vm((NZ, TOK, W), BF16), vm((NS, TOK, W), BF16), vm((TOK, CH), BF16),
        vm((MODEL, 2 * CH), BF16), vm((CH, MODEL), BF16), vm((CH, MODEL), BF16),
        vm((ROWS, TOK), BF16), vm((ROWS, 1), F32),
        vm((ROWS, W), BF16), vm((NZ, ROWS, W), BF16),
        vm((NS, ROWS, W), BF16), vm((NS, ROWS, W), BF16),
        vm((ROWS, 2 * CH), F32), vm((ROWS, CH), F32),
        vm((ROWS, 2 * CH), BF16), vm((ROWS, CH), BF16),
        vm((MODEL, CH), F32), vm((MODEL, CH), F32), vm((CH, MODEL), F32),
        vm((NZ, ROWS, W), BF16), vm((NZ, ROWS, W), BF16),
        vm((2, 4, ROWS, CH), BF16), vm((2, 4, ROWS, CH), BF16),
        vm((NZ, ROWS, CH), BF16), vm((NZ, ROWS, CH), BF16),
        vm((2, 4, TOK, CH), BF16), vm((2, 4, TOK, CH), BF16), vm((TOK, W), F32),
        vm((NZ, ROWS, CH), F32),
        vm((ROWS, CH), BF16), vm((ROWS, CH), BF16),
        vm((NS, TOK, W), BF16), vm((TOK, CH), F32),
        vm((CH, TOK), BF16), vm((TOK, CH), F32), vm((TOK, CH), F32),
        vm((32, CH), F32), vm((32, CH), F32),
        vm((NS, CH, W), BF16), vm((NS, CH, W), BF16),
        vm((3, NS, 8, TOK), F32), vm((3, 8, TOK), F32),
        dma((10,)),
        dma((2, 4, 2)), dma((2, 4, 2)), dma((2, 4, 2)), dma((2, 4, 2)),
        dma((5, 2, 2)), dma((5, 2, 2)),
        dma((1,)), dma((1,)),
        dma((NZ,)), dma((NZ,)), dma((NZ,)), dma((NZ,)),
        dma((NZ,)), dma((NZ,)),
        dma((2, 4, 2)), dma((2, 4, 2)),
        dma((NZ,)), dma((NZ,)), dma((2, 4, 2)), dma((2, 4, 2)),
        dma((2, 4, 2)), dma((2, 4, 2)), dma((5, 2, 2)), dma((5, 2, 2)),
        dma((3,)), dma((3,)),
        dma((1,)), dma((1,)),
        dma((2, 4, 2)), dma((2, 4, 2)), dma((5, 2, 2)), dma((5, 2, 2)),
        dma((1,)), dma((1,)), dma((1,)), dma((1,)),
    ]
    gg, gu, gd, conv_back, out_sum = pl.pallas_call(
        comm_kernel,
        name="exchange",
        out_shape=grads + [shape((TOK + 32, CH), F32), shape((CH, W), F32)],
        in_specs=[near] * 4 + [far] * 7,
        out_specs=[far] * 3 + [near] * 2,
        scratch_shapes=scratch,
        compiler_params=pltpu.CompilerParams(
            collective_id=0, has_side_effects=True, vmem_limit_bytes=67_000_000
        ),
    )(
        norm_gain.reshape(1, W), routes.T, route_weights.T, ln_gain.reshape(1, CH),
        upstream, stream, w_gate[0], w_up[0], w_down[0], conv_pre, w_out,
    )
    grad_gate, grad_up, grad_down, value_grad, gate_grad, grad_out = pl.pallas_call(
        last_kernel,
        name="last",
        out_shape=grads + [shape((TOK, CH), BF16)] * 2 + [shape((CH, W), F32)],
        in_specs=[far] * 3 + [near] * 5,
        out_specs=[far] * 3 + [near] * 3,
        scratch_shapes=[
            vm((2, MODEL, CH), F32), vm((CH, MODEL), F32), dma((12,)), dma((12,)),
        ],
        compiler_params=pltpu.CompilerParams(vmem_limit_bytes=67_000_000),
    )(gg, gu, gd, conv_back, out_sum, conv_taps, value_in, gate_in)
    return (grad_gate[None], grad_up[None], grad_down[None], grad_out, value_grad, gate_grad)


def solution(mesh):
    return jax.shard_map(
        per_device,
        mesh=mesh,
        in_specs=(
            P("sp", "tp"), P("sp", "tp"), P("tp"), P("sp", None), P("sp", None),
            P("sp", None, "tp"), P("sp", None, "tp"), P("sp", "tp", None),
            P("sp", "tp"), P("sp", "tp"), P("sp", "tp"), P("tp"), P(None, "tp"), P("tp", None),
        ),
        out_specs=(
            P("sp", None, "tp"), P("sp", None, "tp"), P("sp", "tp", None),
            P("tp", "sp"), P("sp", "tp"), P("sp", "tp"),
        ),
        check_vma=False,
    )
```

```python
import jax
import jax.numpy as jnp
from jax import lax
from jax.experimental import pallas as pl
from jax.experimental.pallas import tpu as pltpu
from jax.sharding import PartitionSpec as P

MESH = pl.DeviceIdType.MESH
F32, BF16 = jnp.float32, jnp.bfloat16
EPSILON = 1e-06
NZ, NS = 8, 16
TOK, W, CH = 256, 256, 128
CAP, ROWS, HALF = 48, 768, 384
MODEL, CHANNELS, TAPS = 4096, 2048, 31
STEPS = ((0, 0), (0, 1), (1, 0), (1, 1))
OFFSETS = (0, 1, -1, 2, -2, 3, -3, 4)


def dot(a, b, ca, cb):
    return lax.dot_general(a, b, (((ca,), (cb,)), ((), ())), preferred_element_type=F32)


def columns_to_rows(columns):
    lane = lax.broadcasted_iota(jnp.int32, (TOK, 128), 1)
    packed = jnp.zeros((TOK, 128), F32)
    for k, column in enumerate(columns):
        packed = jnp.where(lane == k, column, packed)
    rows = packed.T[0:4, :]
    return jnp.concatenate([rows[:, 0:128], rows[:, 128:TOK]], axis=0)


def rows_to_columns(rows):
    rows = jnp.concatenate([rows[0:4, :], rows[4:8, :]], axis=1)
    return jnp.concatenate([rows, jnp.zeros((124, TOK), F32)], axis=0).T


def silu_slope(values, logistic):
    return logistic * (1.0 + values * (1.0 - logistic))


def comm_kernel(
    gain_ref, routes_ref, rw_ref, lng_ref, up_h, st_h, wg_h, wu_h, wd_h, cp_h, wo_h,
    gg_h, gu_h, gd_h, cb_o, go_o,
    UP, ST, CP, WC, WD, WO, PICK, SW, SI, SC, X, CT, G, A, CAT, ACT, GG, GU, GD,
    SB, SR, RSS, RSR, PB, RB, TSS, TSR, AP, RK, RC, KS, KR, FIN, RET, SG, MB, MO, CEN, SCL, HS, HALO, GOS, GOR, SS, SX,
    ls, ups, upr, xs, xr, dxs, dxr, as_, ar, cs, cr, dcs, dcr, sbs, sbr, rss, rsr, bs, br, tss, tsr,
    ks, kr, es, er, fs, fr, sgs, sgr, dgs, dgr, gs, gr, hs, hr,
):
    sp = lax.axis_index("sp")
    tp = lax.axis_index("tp")
    z = tp // 2
    c = tp % 2
    sibling = (sp, z * 2 + 1 - c)

    def zat(offset):
        return (z + offset + NZ) % NZ

    def zdev(offset):
        return (sp, zat(offset) * 2 + c)

    def mine(offset):
        return zat(offset) * 2 + c

    def other(offset):
        return zat(offset) * 2 + 1 - c

    def remote(src, dst, ssem, rsem, device):
        return pltpu.make_async_remote_copy(
            src_ref=src, dst_ref=dst, send_sem=ssem, recv_sem=rsem,
            device_id=device, device_id_type=MESH,
        )

    def each_peer(body):
        def step(k, carry):
            body((sp + k) % NS)
            return carry

        lax.fori_loop(1, NS, step, 0)

    barrier = pltpu.get_barrier_semaphore()

    def greet(k, carry):
        pl.semaphore_signal(barrier, inc=1, device_id=(sp, (tp + k) % NS), device_id_type=MESH)
        pl.semaphore_signal(barrier, inc=1, device_id=((sp + k) % NS, tp), device_id_type=MESH)
        return carry

    lax.fori_loop(1, NS, greet, 0)
    loads = [
        pltpu.make_async_copy(up_h, UP.at[z], ls.at[0]),
        pltpu.make_async_copy(st_h, ST, ls.at[1]),
        pltpu.make_async_copy(cp_h, CP, ls.at[2]),
        pltpu.make_async_copy(wg_h, WC.at[:, pl.ds(0, CH)], ls.at[3]),
        pltpu.make_async_copy(wu_h, WC.at[:, pl.ds(CH, CH)], ls.at[4]),
        pltpu.make_async_copy(wd_h, WD, ls.at[5]),
        pltpu.make_async_copy(wo_h, WO, ls.at[6]),
    ]
    for load in loads:
        load.start()

    def active(t, d, h):
        return t <= 3 or d == h

    def ring(buf, index, half, ssem, rsem, t, d, h, arriving):
        sign = 1 - 2 * d
        block = buf.at[index(-sign * (t if arriving else t - 1)), pl.ds(h * half, half)]
        return remote(block, block, ssem.at[d, t - 1, h], rsem.at[d, t - 1, h], zdev(sign))

    def ring_send(*args):
        ring(*args, False).start()

    def ring_take(*args):
        ring(*args, True).wait_recv()

    def x_chunks(t):
        if t == 0:
            return [(0, 0, 0), (0, 1, 0)]
        return [(d, h, -t * (1 - 2 * d)) for h in range(2) for d in range(2) if active(t, d, h)]

    def up_take(t):
        for h in range(2):
            for d in range(2):
                if active(t, d, h):
                    ring_take(UP, zat, TOK // 2, ups, upr, t, d, h)
                    if t < 4 and active(t + 1, d, h):
                        ring_send(UP, zat, TOK // 2, ups, upr, t + 1, d, h)

    def exchange_set(n, rows):
        SX[n] = rows
        SS[n, tp] = rows

    def exchange_start(n):
        def step(k, carry):
            peer = (tp + k) % NS
            remote(SX.at[n], SS.at[n, tp], es.at[n], er.at[n], (sp, peer)).start()
            return carry

        lax.fori_loop(1, NS, step, 0)

    def exchange_end(n):
        many = SS.at[n, pl.ds(0, NS - 1)]
        remote(many, many, es.at[n], er.at[n], sibling).wait_recv()
        return rows_to_columns(jnp.sum(SS[n], axis=0))

    def exchange_flush(n):
        many = SS.at[n, pl.ds(0, NS - 1)]
        remote(many, many, es.at[n], er.at[n], sibling).wait_send()

    loads[1].wait()
    loads[2].wait()
    stream = ST[...].astype(F32)
    conv = CP[...].astype(F32)
    exchange_set(
        0,
        columns_to_rows([
            jnp.sum(stream * stream, axis=1, keepdims=True),
            jnp.sum(conv, axis=1, keepdims=True),
            jnp.sum(conv * conv, axis=1, keepdims=True),
        ]),
    )

    first, second = routes_ref[0:1, :], routes_ref[1:2, :]
    names = lax.broadcasted_iota(jnp.int32, (NS, TOK), 0)
    hit0 = (names == first).astype(F32)
    hit1 = (names == second).astype(F32)
    earlier = (
        lax.broadcasted_iota(jnp.int32, (TOK, TOK), 0) < lax.broadcasted_iota(jnp.int32, (TOK, TOK), 1)
    ).astype(F32).astype(BF16)
    rank = dot((hit0 + hit1).astype(BF16), earlier, 1, 0)
    rank0 = jnp.sum(hit0 * rank, axis=0, keepdims=True).astype(jnp.int32)
    rank1 = jnp.sum(hit1 * rank, axis=0, keepdims=True).astype(jnp.int32)
    RK[0:1, :] = rank0
    RK[1:2, :] = rank1
    slot0 = first * CAP + rank0
    slot1 = second * CAP + rank1
    for r in range(3):
        slots = lax.broadcasted_iota(jnp.int32, (TOK, TOK), 0) + r * TOK
        at0, at1 = slots == slot0, slots == slot1
        rows = pl.ds(r * TOK, TOK)
        PICK[rows, :] = jnp.logical_or(at0, at1).astype(F32).astype(BF16)
        SW[rows, :] = jnp.sum(
            jnp.where(at0, rw_ref[0:1, :], 0.0) + jnp.where(at1, rw_ref[1:2, :], 0.0),
            axis=1, keepdims=True,
        )

    def slot_rows(p):
        return pl.ds(pl.multiple_of(p * CAP, 16), CAP)

    def pick_cotangent(offset):
        origin = zat(offset)

        def pick(r, carry):
            rows = pl.ds(pl.multiple_of(r * TOK, TOK), TOK)
            SC[origin, rows, :] = (dot(PICK[rows, :], UP[origin], 1, 0) * SW[rows, :]).astype(BF16)
            return carry

        lax.fori_loop(0, 3, pick, 0)

    def send_cotangent(offset):
        origin = zat(offset)
        block = mine(offset)

        def send(p):
            remote(
                SC.at[origin, slot_rows(p)], CT.at[block, slot_rows(sp)],
                cs.at[origin], cr.at[origin], (p, tp),
            ).start()

        each_peer(send)
        CT[block, slot_rows(sp), :] = SC[origin, slot_rows(sp), :]

    def cotangent(offset):
        pick_cotangent(offset)
        send_cotangent(offset)

    loads[0].wait()
    pick_cotangent(0)
    pl.semaphore_wait(barrier, 2 * (NS - 1))
    exchange_start(0)
    for h in range(2):
        for d in range(2):
            ring_send(UP, zat, TOK // 2, ups, upr, 1, d, h)
    send_cotangent(0)
    stats = exchange_end(0)
    inverse = lax.rsqrt(stats[:, 0:1] / MODEL + EPSILON)
    mean_val = stats[:, 1:2] / CHANNELS
    inv_std = lax.rsqrt(stats[:, 2:3] / CHANNELS - mean_val * mean_val + EPSILON)
    normed = (gain_ref[...] * ST[...].astype(F32) * inverse).astype(BF16)
    for r in range(3):
        rows = pl.ds(r * TOK, TOK)
        SI[rows, :] = dot(PICK[rows, :], normed, 1, 0).astype(BF16)
    own = mine(0)

    def send_input(p):
        remote(SI.at[slot_rows(p)], X.at[own, slot_rows(sp)], as_.at[0], ar.at[0], (p, tp)).start()

    each_peer(send_input)
    X[own, slot_rows(sp), :] = SI[slot_rows(sp), :]

    up_take(1)
    cotangent(1)
    cotangent(-1)
    up_take(2)
    centred = (CP[...].astype(F32) - mean_val) * inv_std
    scaled = centred * lng_ref[...]
    CEN[...] = centred
    SCL[...] = scaled
    MO[...] = (scaled * jax.nn.sigmoid(scaled)).T.astype(BF16)
    G[...] = jnp.zeros_like(G)
    A[...] = jnp.zeros_like(A)

    for k in range(3, 6):
        loads[k].wait()

    def take_many(dst, ssem, rsem):
        remote(dst, dst, ssem, rsem, sibling).wait_recv()

    def flush_many(src, ssem, rsem):
        remote(src, src, ssem, rsem, sibling).wait_send()

    def cols(j):
        return pl.ds(pl.multiple_of(j * W, W), W)

    def add_inputs(blocks):
        total = G[...]
        for j in blocks:
            total = total + dot(X[j], WC[cols(j), :], 1, 0)
        G[...] = total

    def add_cotangents(blocks):
        total = A[...]
        for j in blocks:
            total = total + dot(CT[j], WD[:, cols(j)], 1, 1)
        A[...] = total

    def hand_over(t, d, h, offset, arriving):
        j = other(offset) if arriving else mine(offset)
        block = X.at[j, pl.ds(h * HALF, HALF)]
        return remote(block, block, dxs.at[t, d, h], dxr.at[t, d, h], sibling)

    def x_ring(t, d, h):
        return (X, mine, HALF, xs, xr, t, d, h)

    def hand_cotangent(offset, arriving):
        j = other(offset) if arriving else mine(offset)
        return remote(CT.at[j], CT.at[j], dcs.at[zat(offset)], dcr.at[zat(offset)], sibling)

    take_many(X.at[own, pl.ds(0, ROWS - CAP)], as_.at[0], ar.at[0])
    for d, h in STEPS:
        ring_send(*x_ring(1, d, h))
    for h in range(2):
        hand_over(0, 0, h, 0, False).start()
    add_inputs([own])
    cotangent(2)
    cotangent(-2)
    up_take(3)
    cotangent(3)
    cotangent(-3)

    def stage_offsets(t):
        return (0,) if t == 0 else ((t, -t) if t < 4 else (4,))

    def from_sibling(t):
        for d, h, offset in x_chunks(t):
            hand_over(t, d, h, offset, True).wait_recv()
        add_inputs([other(offset) for offset in stage_offsets(t)])

    def cot_own(offsets):
        for offset in offsets:
            take_many(CT.at[mine(offset), pl.ds(0, ROWS - CAP)], cs.at[zat(offset)], cr.at[zat(offset)])
            hand_cotangent(offset, False).start()
        add_cotangents([mine(offset) for offset in offsets])

    def cot_other(offsets):
        for offset in offsets:
            hand_cotangent(offset, True).wait_recv()
        add_cotangents([other(offset) for offset in offsets])

    cot_stages = ((0, 1), (-1, 2, -2), (3, -3), (4,))
    for t in range(1, 5):
        for d, h, offset in x_chunks(t):
            ring_take(*x_ring(t, d, h))
            if t < 4 and active(t + 1, d, h):
                ring_send(*x_ring(t + 1, d, h))
            hand_over(t, d, h, offset, False).start()
        if t == 1:
            up_take(4)
            cotangent(4)
        add_inputs([mine(offset) for offset in stage_offsets(t)])
        from_sibling(t - 1)
        cot_own(cot_stages[t - 1])
        if t > 1:
            cot_other(cot_stages[t - 2])
    from_sibling(4)
    cot_other(cot_stages[3])

    def hidden(r, carry):
        rows = pl.ds(pl.multiple_of(r * 64, 64), 64)
        gate, upper, back = G[rows, 0:CH], G[rows, CH : 2 * CH], A[rows, :]
        logistic = jax.nn.sigmoid(gate)
        silu = gate * logistic
        ACT[rows, :] = (silu * upper).astype(BF16)
        gate_back = (back * upper * silu_slope(gate, logistic)).astype(BF16)
        upper_back = (back * silu).astype(BF16)
        CAT[rows, 0:CH] = gate_back
        CAT[rows, CH : 2 * CH] = upper_back
        return carry

    lax.fori_loop(0, 12, hidden, 0)

    def send_sums():
        def row_sums(r, carry):
            rows = pl.ds(pl.multiple_of(r * 64, 64), 64)
            RC[rows, :] = jnp.sum(CAT[rows, :].astype(F32) * G[rows, :], axis=1, keepdims=True)
            return carry

        lax.fori_loop(0, 12, row_sums, 0)
        slot_lane = lax.broadcasted_iota(jnp.int32, (CAP, 128), 0) == lax.broadcasted_iota(
            jnp.int32, (CAP, 128), 1
        )
        top = lax.broadcasted_iota(jnp.int32, (8, 128), 0) == 0
        for p in range(NS):
            row = jnp.sum(jnp.where(slot_lane, RC[p * CAP : p * CAP + CAP, :], 0.0), axis=0, keepdims=True)
            KS[p] = jnp.where(top, row, 0.0)

        def send(p):
            remote(KS.at[p], KR.at[sp], ks.at[0], kr.at[0], (p, tp)).start()

        each_peer(send)
        KR[sp] = KS[sp]

    def inner_sums():
        take_many(KR.at[pl.ds(0, NS - 1)], ks.at[0], kr.at[0])
        by_slot = jnp.sum(KR[...], axis=1)
        names = lax.broadcasted_iota(jnp.int32, (NS, TOK), 0)
        ranks = lax.broadcasted_iota(jnp.int32, (128, TOK), 0)
        total = jnp.zeros((1, TOK), F32)
        for k in range(2):
            picked = lax.dot_general(
                by_slot, (ranks == RK[k : k + 1, :]).astype(F32), (((1,), (0,)), ((), ())),
                precision=lax.Precision.HIGHEST, preferred_element_type=F32,
            )
            total = total + jnp.sum(
                jnp.where(names == routes_ref[k : k + 1, :], picked, 0.0), axis=0, keepdims=True
            )
        row = lax.broadcasted_iota(jnp.int32, (8, 128), 0)
        exchange_set(
            1, jnp.where(row == 0, total[:, 0:128], jnp.where(row == 4, total[:, 128:TOK], 0.0))
        )
        exchange_start(1)

    def for_sibling(offset):
        q = zat(offset)
        j = other(offset)

        SB[q] = dot(CAT[...], WC[cols(j), :], 1, 1).astype(BF16)
        remote(SB.at[q], SR.at[q], sbs.at[q], sbr.at[q], sibling).start()

    def take_sibling(offset):
        q = zat(offset)
        remote(SB.at[q], SR.at[q], sbs.at[q], sbr.at[q], sibling).wait_recv()

    def chip_part(offset):
        q = zat(offset)
        take_sibling(offset)
        part = dot(CAT[...], WC[cols(mine(offset)), :], 1, 1) + SR[q].astype(F32)
        AP[q] = part[:, 0:CH]
        PB[q] = part[:, CH : 2 * CH].astype(BF16)

        def send(p):
            remote(PB.at[q, slot_rows(p)], RB.at[q, slot_rows(sp)], bs.at[q], br.at[q], (p, tp)).start()

        each_peer(send)
        RB[q, slot_rows(sp), :] = PB[q, slot_rows(sp), :]

    def rs_copy(d, k, h):
        part = pl.ds(h * HALF, HALF)
        return remote(
            RSS.at[d, k, part], RSR.at[d, k, part], rss.at[d, k, h], rsr.at[d, k, h], zdev(1 - 2 * d)
        )

    def rs_active(k, d, h):
        return k >= 1 or d == h

    def rs_send(k, d, h):
        offset = (4 - k) * (1 - 2 * d)
        incoming = k >= 1 and rs_active(k - 1, d, h)
        if incoming:
            rs_copy(d, k - 1, h).wait_recv()

        part = slice(h * HALF, h * HALF + HALF)
        total = AP[zat(offset), part, :]
        if incoming:
            total = total + RSR[d, k - 1, part, :].astype(F32)
        RSS[d, k, part, :] = total.astype(BF16)
        rs_copy(d, k, h).start()

    def back_take(offset):
        q = zat(offset)
        take_many(RB.at[q, pl.ds(0, ROWS - CAP)], bs.at[q], br.at[q])

    def token_part(offset, h):
        return dot(PICK[:, h * CH : h * CH + CH], RB[zat(offset)], 0, 0)

    def ts_copy(d, k, h):
        part = pl.ds(h * CH, CH)
        return remote(
            TSS.at[d, k, part], TSR.at[d, k, part], tss.at[d, k, h], tsr.at[d, k, h], zdev(1 - 2 * d)
        )

    def ts_send(k, d, h):
        total = token_part((4 - k) * (1 - 2 * d), h)
        if k >= 1 and rs_active(k - 1, d, h):
            ts_copy(d, k - 1, h).wait_recv()
            total = total + TSR[d, k - 1, h * CH : h * CH + CH, :].astype(F32)
        TSS[d, k, h * CH : h * CH + CH, :] = total.astype(BF16)
        ts_copy(d, k, h).start()

    def ts_step(k):
        for offset in stage_offsets(4 - k):
            back_take(offset)
        for d, h in ((0, 1), (1, 0), (0, 0), (1, 1)):
            if rs_active(k, d, h):
                ts_send(k, d, h)

    def rs_step(k):
        for d, h in ((0, 1), (1, 0), (0, 0), (1, 1)):
            if rs_active(k, d, h):
                rs_send(k, d, h)

    def gradients(first_block):
        def step(b, carry):
            j = first_block + b
            both = dot(X[j], CAT[...], 0, 0)
            GG[cols(j), :] = both[:, 0:CH]
            GU[cols(j), :] = both[:, CH : 2 * CH]
            GD[:, cols(j)] = dot(ACT[...], CT[j], 0, 0)
            return carry

        lax.fori_loop(0, 4, step, 0)

    for_sibling(4)
    for_sibling(3)
    for_sibling(-3)
    chip_part(4)
    rs_step(0)
    send_sums()
    chip_part(3)
    chip_part(-3)
    for_sibling(2)
    for_sibling(-2)
    rs_step(1)
    chip_part(2)
    chip_part(-2)
    for_sibling(1)
    for_sibling(-1)
    for_sibling(0)
    rs_step(2)
    inner_sums()
    ts_step(0)
    chip_part(1)
    chip_part(-1)
    gradients(0)
    rs_step(3)
    chip_part(0)
    ts_step(1)
    gradients(4)
    for h in range(2):
        rs_copy(0, 3, h).wait_recv()
        rs_copy(1, 3, h).wait_recv()

        part = slice(h * HALF, h * HALF + HALF)
        FIN[part, :] = (
            AP[z, part, :] + RSR[0, 3, part, :].astype(F32) + RSR[1, 3, part, :].astype(F32)
        ).astype(BF16)

    def send_back(p):
        remote(FIN.at[slot_rows(p)], RET.at[slot_rows(sp)], fs.at[0], fr.at[0], (p, tp)).start()

    each_peer(send_back)
    RET[slot_rows(sp), :] = FIN[slot_rows(sp), :]
    ts_step(2)
    gradients(8)
    ts_step(3)
    def sg_ring(t, d, h, arriving):
        sign = 1 - 2 * d
        block = SG.at[mine(-sign * (t if arriving else t - 1)), :, pl.ds(h * CH, CH)]
        return remote(block, block, sgs.at[d, t - 1, h], sgr.at[d, t - 1, h], zdev(sign))

    def sg_hand(t, d, h, offset, arriving):
        block = SG.at[other(offset) if arriving else mine(offset), :, pl.ds(h * CH, CH)]
        return remote(block, block, dgs.at[t, d, h], dgr.at[t, d, h], sibling)

    def sg_first(h, token_back):
        part = slice(h * CH, h * CH + CH)
        SG[own, :, part] = (
            UP[z, :, part].astype(F32)
            + inverse * gain_ref[:, part] * token_back
            - ST[:, part].astype(F32) * share
        ).astype(BF16)
        for d in range(2):
            sg_ring(1, d, h, False).start()
        sg_hand(0, 0, h, 0, False).start()

    share = inverse * inverse * (exchange_end(1)[:, 0:1] / MODEL)
    take_many(RET.at[pl.ds(0, ROWS - CAP)], fs.at[0], fr.at[0])
    sg_first(0, dot(PICK[...], RET[...], 0, 0))
    back_take(0)
    finals = []
    for h in range(2):
        total = token_part(0, h)
        for d in range(2):
            ts_copy(d, 3, h).wait_recv()
            total = total + TSR[d, 3, h * CH : h * CH + CH, :].astype(F32)
        finals.append(total)
    sg_first(1, jnp.concatenate(finals, axis=0))
    loads[6].wait()

    def mix(j):
        block = SG[j]
        part = dot(MO[...], block, 1, 0).astype(BF16)

        @pl.when(j == sp)
        def _():
            GOR[sp] = part

        @pl.when(j != sp)
        def _():
            GOS[j] = part
            remote(GOS.at[j], GOR.at[sp], gs.at[0], gr.at[0], (j, tp)).start()

        MB[...] = MB[...] + dot(block, WO[:, cols(j)], 1, 1)

    MB[...] = jnp.zeros_like(MB)
    mix(own)

    def mix_other(t):
        for d, h, offset in x_chunks(t):
            sg_hand(t, d, h, offset, True).wait_recv()
        for offset in stage_offsets(t):
            mix(other(offset))

    for t in range(1, 5):
        for d, h, offset in x_chunks(t):
            sg_ring(t, d, h, True).wait_recv()
            if t < 4 and active(t + 1, d, h):
                sg_ring(t + 1, d, h, False).start()
            sg_hand(t, d, h, offset, False).start()
        for offset in stage_offsets(t):
            mix(mine(offset))
        mix_other(t - 1)
    mix_other(4)

    scaled = SCL[...]
    norm_in = MB[...] * silu_slope(scaled, jax.nn.sigmoid(scaled)) * lng_ref[...]
    exchange_set(
        2,
        columns_to_rows([
            jnp.sum(norm_in, axis=1, keepdims=True),
            jnp.sum(norm_in * CEN[...], axis=1, keepdims=True),
        ]),
    )
    exchange_start(2)

    gradients(12)
    stores = [
        pltpu.make_async_copy(GG, gg_h, ls.at[7]),
        pltpu.make_async_copy(GU, gu_h, ls.at[8]),
        pltpu.make_async_copy(GD, gd_h, ls.at[9]),
    ]
    for store in stores:
        store.start()
    sums = exchange_end(2)
    conv_back = inv_std * (
        norm_in - sums[:, 0:1] / CHANNELS - CEN[...] * (sums[:, 1:2] / CHANNELS)
    )
    HS[...] = conv_back[0:32, :]
    previous = ((sp + NS - 1) % NS, tp)

    @pl.when(sp > 0)
    def _():
        remote(HS, HALO, hs.at[0], hr.at[0], previous).start()

    cb_o[0:TOK, :] = conv_back

    @pl.when(sp < NS - 1)
    def _():
        remote(HS, HALO, hs.at[0], hr.at[0], previous).wait_recv()
        cb_o[TOK : TOK + 32, :] = HALO[...]

    @pl.when(sp == NS - 1)
    def _():
        cb_o[TOK : TOK + 32, :] = jnp.zeros((32, CH), F32)

    take_many(GOR.at[pl.ds(0, NS - 1)], gs.at[0], gr.at[0])

    def total(i, acc):
        return acc + GOR[i].astype(F32)

    go_o[...] = lax.fori_loop(0, NS, total, jnp.zeros((CH, W), F32))

    for t in range(1, 5):
        for d, h in STEPS:
            if active(t, d, h):
                ring(UP, zat, TOK // 2, ups, upr, t, d, h, False).wait_send()
                ring(*x_ring(t, d, h), False).wait_send()
                sg_ring(t, d, h, False).wait_send()
    for t in range(5):
        for d, h, offset in x_chunks(t):
            hand_over(t, d, h, offset, False).wait_send()
            sg_hand(t, d, h, offset, False).wait_send()
    for offset in OFFSETS:
        q = zat(offset)
        flush_many(SC.at[q, pl.ds(0, ROWS - CAP)], cs.at[q], cr.at[q])
        hand_cotangent(offset, False).wait_send()
        flush_many(PB.at[q, pl.ds(0, ROWS - CAP)], bs.at[q], br.at[q])
        remote(SB.at[q], SR.at[q], sbs.at[q], sbr.at[q], sibling).wait_send()
    for k in range(4):
        for d, h in STEPS:
            if rs_active(k, d, h):
                rs_copy(d, k, h).wait_send()
                ts_copy(d, k, h).wait_send()
    for n in range(3):
        exchange_flush(n)
    flush_many(KS.at[pl.ds(0, NS - 1)], ks.at[0], kr.at[0])
    flush_many(SI.at[pl.ds(0, ROWS - CAP)], as_.at[0], ar.at[0])
    flush_many(FIN.at[pl.ds(0, ROWS - CAP)], fs.at[0], fr.at[0])
    flush_many(GOS.at[pl.ds(0, NS - 1)], gs.at[0], gr.at[0])

    @pl.when(sp > 0)
    def _():
        remote(HS, HALO, hs.at[0], hr.at[0], previous).wait_send()

    for store in stores:
        store.wait()


def last_kernel(
    gg_i, gu_i, gd_i, cb_ref, go_ref, taps_ref, value_ref, gate_ref,
    gg_o, gu_o, gd_o, vg_o, tg_o, go_o, bufs_tall, buf_wide, lsem, ssem,
):
    pieces = []
    for a, (src, dst) in enumerate(((gg_i, gg_o), (gu_i, gu_o))):
        for q in range(4):
            part = pl.ds(q * 1024, 1024)
            pieces.append((src.at[part], bufs_tall.at[a, part], dst.at[part]))
    for q in range(4):
        part = pl.ds(q * 32, 32)
        pieces.append((gd_i.at[part], buf_wide.at[part], gd_o.at[part]))
    ins = [pltpu.make_async_copy(s, b, lsem.at[n]) for n, (s, b, _) in enumerate(pieces)]
    outs = [pltpu.make_async_copy(b, d, ssem.at[n]) for n, (_, b, d) in enumerate(pieces)]
    for copy in ins:
        copy.start()
    for i, o in zip(ins, outs):
        i.wait()
        o.start()
    go_o[...] = go_ref[...]
    acc = jnp.zeros((TOK, CH), F32)
    for tap in range(TAPS):
        acc = acc + taps_ref[tap : tap + 1, :] * cb_ref[TAPS - 1 - tap : TAPS - 1 - tap + TOK, :]
    sigma = jax.nn.sigmoid(gate_ref[...].astype(F32))
    vg_o[...] = (acc * sigma).astype(BF16)
    tg_o[...] = (acc * value_ref[...].astype(F32) * sigma * (1.0 - sigma)).astype(BF16)
    for copy in outs:
        copy.wait()


def shape(dims, dtype):
    return jax.ShapeDtypeStruct(dims, dtype)


def per_device(
    upstream, stream, norm_gain, routes, route_weights, w_gate, w_up, w_down,
    value_in, gate_in, conv_pre, ln_gain, conv_taps, w_out,
):
    near, far = pl.BlockSpec(memory_space=pltpu.VMEM), pl.BlockSpec(memory_space=pl.ANY)
    dma, vm = pltpu.SemaphoreType.DMA, pltpu.VMEM
    grads = [shape((MODEL, CH), F32), shape((MODEL, CH), F32), shape((CH, MODEL), F32)]
    scratch = [
        vm((NZ, TOK, W), BF16), vm((TOK, W), BF16), vm((TOK, CH), BF16),
        vm((MODEL, 2 * CH), BF16), vm((CH, MODEL), BF16), vm((CH, MODEL), BF16),
        vm((ROWS, TOK), BF16), vm((ROWS, 1), F32),
        vm((ROWS, W), BF16), vm((NZ, ROWS, W), BF16),
        vm((NS, ROWS, W), BF16), vm((NS, ROWS, W), BF16),
        vm((ROWS, 2 * CH), F32), vm((ROWS, CH), F32),
        vm((ROWS, 2 * CH), BF16), vm((ROWS, CH), BF16),
        vm((MODEL, CH), F32), vm((MODEL, CH), F32), vm((CH, MODEL), F32),
        vm((NZ, ROWS, W), BF16), vm((NZ, ROWS, W), BF16),
        vm((2, 4, ROWS, CH), BF16), vm((2, 4, ROWS, CH), BF16),
        vm((NZ, ROWS, CH), BF16), vm((NZ, ROWS, CH), BF16),
        vm((2, 4, TOK, CH), BF16), vm((2, 4, TOK, CH), BF16),
        vm((NZ, ROWS, CH), F32), vm((8, TOK), jnp.int32), vm((ROWS, 1), F32),
        vm((NS, 8, 128), F32), vm((NS, 8, 128), F32),
        vm((ROWS, CH), BF16), vm((ROWS, CH), BF16),
        vm((NS, TOK, W), BF16), vm((TOK, CH), F32),
        vm((CH, TOK), BF16), vm((TOK, CH), F32), vm((TOK, CH), F32),
        vm((32, CH), F32), vm((32, CH), F32),
        vm((NS, CH, W), BF16), vm((NS, CH, W), BF16),
        vm((3, NS, 8, 128), F32), vm((3, 8, 128), F32),
        dma((10,)),
        dma((2, 4, 2)), dma((2, 4, 2)), dma((2, 4, 2)), dma((2, 4, 2)),
        dma((5, 2, 2)), dma((5, 2, 2)),
        dma((1,)), dma((1,)),
        dma((NZ,)), dma((NZ,)), dma((NZ,)), dma((NZ,)),
        dma((NZ,)), dma((NZ,)),
        dma((2, 4, 2)), dma((2, 4, 2)),
        dma((NZ,)), dma((NZ,)), dma((2, 4, 2)), dma((2, 4, 2)),
        dma((1,)), dma((1,)),
        dma((3,)), dma((3,)),
        dma((1,)), dma((1,)),
        dma((2, 4, 2)), dma((2, 4, 2)), dma((5, 2, 2)), dma((5, 2, 2)),
        dma((1,)), dma((1,)), dma((1,)), dma((1,)),
    ]
    gg, gu, gd, conv_back, out_sum = pl.pallas_call(
        comm_kernel,
        name="exchange",
        out_shape=grads + [shape((TOK + 32, CH), F32), shape((CH, W), F32)],
        in_specs=[near] * 4 + [far] * 7,
        out_specs=[far] * 3 + [near] * 2,
        scratch_shapes=scratch,
        compiler_params=pltpu.CompilerParams(
            collective_id=0, has_side_effects=True, vmem_limit_bytes=67_000_000
        ),
    )(
        norm_gain.reshape(1, W), routes.T, route_weights.T, ln_gain.reshape(1, CH),
        upstream, stream, w_gate[0], w_up[0], w_down[0], conv_pre, w_out,
    )
    grad_gate, grad_up, grad_down, value_grad, gate_grad, grad_out = pl.pallas_call(
        last_kernel,
        name="last",
        out_shape=grads + [shape((TOK, CH), BF16)] * 2 + [shape((CH, W), F32)],
        in_specs=[far] * 3 + [near] * 5,
        out_specs=[far] * 3 + [near] * 3,
        scratch_shapes=[
            vm((2, MODEL, CH), F32), vm((CH, MODEL), F32), dma((12,)), dma((12,)),
        ],
        compiler_params=pltpu.CompilerParams(vmem_limit_bytes=67_000_000),
    )(gg, gu, gd, conv_back, out_sum, conv_taps, value_in, gate_in)
    return (grad_gate[None], grad_up[None], grad_down[None], grad_out, value_grad, gate_grad)


def solution(mesh):
    return jax.shard_map(
        per_device,
        mesh=mesh,
        in_specs=(
            P("sp", "tp"), P("sp", "tp"), P("tp"), P("sp", None), P("sp", None),
            P("sp", None, "tp"), P("sp", None, "tp"), P("sp", "tp", None),
            P("sp", "tp"), P("sp", "tp"), P("sp", "tp"), P("tp"), P(None, "tp"), P("tp", None),
        ),
        out_specs=(
            P("sp", None, "tp"), P("sp", None, "tp"), P("sp", "tp", None),
            P("tp", "sp"), P("sp", "tp"), P("sp", "tp"),
        ),
        check_vma=False,
    )
```

```python
import jax
import jax.numpy as jnp
from jax import lax
from jax.experimental import pallas as pl
from jax.experimental.pallas import tpu as pltpu
from jax.sharding import PartitionSpec as P

MESH = pl.DeviceIdType.MESH
F32, BF16 = jnp.float32, jnp.bfloat16
EPSILON = 1e-06
NZ, NS = 8, 16
TOK, W, CH = 256, 256, 128
CAP, ROWS, HALF = 48, 768, 384
MODEL, CHANNELS, TAPS = 4096, 2048, 31
STEPS = ((0, 0), (0, 1), (1, 0), (1, 1))
OFFSETS = (0, 1, -1, 2, -2, 3, -3, 4)


def dot(a, b, ca, cb):
    return lax.dot_general(a, b, (((ca,), (cb,)), ((), ())), preferred_element_type=F32)


def columns_to_rows(columns):
    lane = lax.broadcasted_iota(jnp.int32, (TOK, 128), 1)
    packed = jnp.zeros((TOK, 128), F32)
    for k, column in enumerate(columns):
        packed = jnp.where(lane == k, column, packed)
    rows = packed.T[0:4, :]
    return jnp.concatenate([rows[:, 0:128], rows[:, 128:TOK]], axis=0)


def rows_to_columns(rows):
    rows = jnp.concatenate([rows[0:4, :], rows[4:8, :]], axis=1)
    return jnp.concatenate([rows, jnp.zeros((124, TOK), F32)], axis=0).T


def silu_slope(values, logistic):
    return logistic * (1.0 + values * (1.0 - logistic))


def comm_kernel(
    gain_ref, routes_ref, rw_ref, lng_ref, up_h, st_h, wg_h, wu_h, wd_h, cp_h, wo_h,
    gg_h, gu_h, gd_h, cb_o, go_o,
    UP, ST, CP, WC, WD, WO, PICK, SW, SI, SC, X, CT, G, A, CAT, ACT, GG, GU, GD,
    SB, SR, RSS, RSR, PB, RB, TSS, TSR, AP, RK, RC, KS, KR, FIN, RET, SG, MB, MO, CEN, SCL, HS, HALO, GOS, GOR, SS, SX,
    ls, ups, upr, xs, xr, dxs, dxr, as_, ar, cs, cr, dcs, dcr, sbs, sbr, rss, rsr, bs, br, tss, tsr,
    ks, kr, es, er, fs, fr, sgs, sgr, dgs, dgr, gs, gr, hs, hr,
):
    sp = lax.axis_index("sp")
    tp = lax.axis_index("tp")
    z = tp // 2
    c = tp % 2
    sibling = (sp, z * 2 + 1 - c)

    def zat(offset):
        return (z + offset + NZ) % NZ

    def zdev(offset):
        return (sp, zat(offset) * 2 + c)

    def mine(offset):
        return zat(offset) * 2 + c

    def other(offset):
        return zat(offset) * 2 + 1 - c

    def remote(src, dst, ssem, rsem, device):
        return pltpu.make_async_remote_copy(
            src_ref=src, dst_ref=dst, send_sem=ssem, recv_sem=rsem,
            device_id=device, device_id_type=MESH,
        )

    def each_peer(body):
        def step(k, carry):
            body((sp + k) % NS)
            return carry

        lax.fori_loop(1, NS, step, 0)

    barrier = pltpu.get_barrier_semaphore()

    def greet(k, carry):
        pl.semaphore_signal(barrier, inc=1, device_id=(sp, (tp + k) % NS), device_id_type=MESH)
        pl.semaphore_signal(barrier, inc=1, device_id=((sp + k) % NS, tp), device_id_type=MESH)
        return carry

    lax.fori_loop(1, NS, greet, 0)
    loads = [
        pltpu.make_async_copy(up_h, UP.at[z], ls.at[0]),
        pltpu.make_async_copy(st_h, ST, ls.at[1]),
        pltpu.make_async_copy(cp_h, CP, ls.at[2]),
        pltpu.make_async_copy(wg_h, WC.at[:, pl.ds(0, CH)], ls.at[3]),
        pltpu.make_async_copy(wu_h, WC.at[:, pl.ds(CH, CH)], ls.at[4]),
        pltpu.make_async_copy(wd_h, WD, ls.at[5]),
        pltpu.make_async_copy(wo_h, WO, ls.at[6]),
    ]
    for load in loads:
        load.start()

    def active(t, d, h):
        return t <= 3 or d == h

    def ring(buf, index, half, ssem, rsem, t, d, h, arriving):
        sign = 1 - 2 * d
        block = buf.at[index(-sign * (t if arriving else t - 1)), pl.ds(h * half, half)]
        return remote(block, block, ssem.at[d, t - 1, h], rsem.at[d, t - 1, h], zdev(sign))

    def ring_send(*args):
        ring(*args, False).start()

    def ring_take(*args):
        ring(*args, True).wait_recv()

    def x_chunks(t):
        if t == 0:
            return [(0, 0, 0), (0, 1, 0)]
        return [(d, h, -t * (1 - 2 * d)) for h in range(2) for d in range(2) if active(t, d, h)]

    def up_take(t):
        for h in range(2):
            for d in range(2):
                if active(t, d, h):
                    ring_take(UP, zat, TOK // 2, ups, upr, t, d, h)
                    if t < 4 and active(t + 1, d, h):
                        ring_send(UP, zat, TOK // 2, ups, upr, t + 1, d, h)

    def exchange_set(n, rows):
        SX[n] = rows
        SS[n, tp] = rows

    def exchange_start(n):
        def step(k, carry):
            peer = (tp + k) % NS
            remote(SX.at[n], SS.at[n, tp], es.at[n], er.at[n], (sp, peer)).start()
            return carry

        lax.fori_loop(1, NS, step, 0)

    def exchange_end(n):
        many = SS.at[n, pl.ds(0, NS - 1)]
        remote(many, many, es.at[n], er.at[n], sibling).wait_recv()
        return rows_to_columns(jnp.sum(SS[n], axis=0))

    def exchange_flush(n):
        many = SS.at[n, pl.ds(0, NS - 1)]
        remote(many, many, es.at[n], er.at[n], sibling).wait_send()

    loads[1].wait()
    loads[2].wait()
    stream = ST[...].astype(F32)
    conv = CP[...].astype(F32)
    exchange_set(
        0,
        columns_to_rows([
            jnp.sum(stream * stream, axis=1, keepdims=True),
            jnp.sum(conv, axis=1, keepdims=True),
            jnp.sum(conv * conv, axis=1, keepdims=True),
        ]),
    )

    first, second = routes_ref[0:1, :], routes_ref[1:2, :]
    names = lax.broadcasted_iota(jnp.int32, (NS, TOK), 0)
    hit0 = (names == first).astype(F32)
    hit1 = (names == second).astype(F32)
    earlier = (
        lax.broadcasted_iota(jnp.int32, (TOK, TOK), 0) < lax.broadcasted_iota(jnp.int32, (TOK, TOK), 1)
    ).astype(F32).astype(BF16)
    rank = dot((hit0 + hit1).astype(BF16), earlier, 1, 0)
    rank0 = jnp.sum(hit0 * rank, axis=0, keepdims=True).astype(jnp.int32)
    rank1 = jnp.sum(hit1 * rank, axis=0, keepdims=True).astype(jnp.int32)
    RK[0:1, :] = rank0
    RK[1:2, :] = rank1
    slot0 = first * CAP + rank0
    slot1 = second * CAP + rank1
    for r in range(3):
        slots = lax.broadcasted_iota(jnp.int32, (TOK, TOK), 0) + r * TOK
        at0, at1 = slots == slot0, slots == slot1
        rows = pl.ds(r * TOK, TOK)
        PICK[rows, :] = jnp.logical_or(at0, at1).astype(F32).astype(BF16)
        SW[rows, :] = jnp.sum(
            jnp.where(at0, rw_ref[0:1, :], 0.0) + jnp.where(at1, rw_ref[1:2, :], 0.0),
            axis=1, keepdims=True,
        )

    def slot_rows(p):
        return pl.ds(pl.multiple_of(p * CAP, 16), CAP)

    def pick_cotangent(offset):
        origin = zat(offset)

        SC[origin] = (dot(PICK[...], UP[origin], 1, 0) * SW[...]).astype(BF16)

    def send_cotangent(offset):
        origin = zat(offset)
        block = mine(offset)

        def send(p):
            remote(
                SC.at[origin, slot_rows(p)], CT.at[block, slot_rows(sp)],
                cs.at[origin], cr.at[origin], (p, tp),
            ).start()

        each_peer(send)
        CT[block, slot_rows(sp), :] = SC[origin, slot_rows(sp), :]

    def cotangent(offset):
        pick_cotangent(offset)
        send_cotangent(offset)

    loads[0].wait()
    pick_cotangent(0)
    pl.semaphore_wait(barrier, 2 * (NS - 1))
    exchange_start(0)
    for h in range(2):
        for d in range(2):
            ring_send(UP, zat, TOK // 2, ups, upr, 1, d, h)
    send_cotangent(0)
    stats = exchange_end(0)
    inverse = lax.rsqrt(stats[:, 0:1] / MODEL + EPSILON)
    mean_val = stats[:, 1:2] / CHANNELS
    inv_std = lax.rsqrt(stats[:, 2:3] / CHANNELS - mean_val * mean_val + EPSILON)
    normed = (gain_ref[...] * ST[...].astype(F32) * inverse).astype(BF16)
    for r in range(3):
        rows = pl.ds(r * TOK, TOK)
        SI[rows, :] = dot(PICK[rows, :], normed, 1, 0).astype(BF16)
    own = mine(0)

    def send_input(p):
        remote(SI.at[slot_rows(p)], X.at[own, slot_rows(sp)], as_.at[0], ar.at[0], (p, tp)).start()

    each_peer(send_input)
    X[own, slot_rows(sp), :] = SI[slot_rows(sp), :]

    up_take(1)
    up_take(2)
    centred = (CP[...].astype(F32) - mean_val) * inv_std
    scaled = centred * lng_ref[...]
    CEN[...] = centred
    SCL[...] = scaled
    MO[...] = (scaled * jax.nn.sigmoid(scaled)).T.astype(BF16)
    G[...] = jnp.zeros_like(G)
    A[...] = jnp.zeros_like(A)

    for k in range(3, 6):
        loads[k].wait()

    def take_many(dst, ssem, rsem):
        remote(dst, dst, ssem, rsem, sibling).wait_recv()

    def flush_many(src, ssem, rsem):
        remote(src, src, ssem, rsem, sibling).wait_send()

    def cols(j):
        return pl.ds(pl.multiple_of(j * W, W), W)

    def add_inputs(blocks):
        total = G[...]
        for j in blocks:
            total = total + dot(X[j], WC[cols(j), :], 1, 0)
        G[...] = total

    def add_cotangents(blocks):
        total = A[...]
        for j in blocks:
            total = total + dot(CT[j], WD[:, cols(j)], 1, 1)
        A[...] = total

    def hand_over(t, d, h, offset, arriving):
        j = other(offset) if arriving else mine(offset)
        block = X.at[j, pl.ds(h * HALF, HALF)]
        return remote(block, block, dxs.at[t, d, h], dxr.at[t, d, h], sibling)

    def x_ring(t, d, h):
        return (X, mine, HALF, xs, xr, t, d, h)

    def hand_cotangent(offset, arriving):
        j = other(offset) if arriving else mine(offset)
        return remote(CT.at[j], CT.at[j], dcs.at[zat(offset)], dcr.at[zat(offset)], sibling)

    take_many(X.at[own, pl.ds(0, ROWS - CAP)], as_.at[0], ar.at[0])
    for d, h in STEPS:
        ring_send(*x_ring(1, d, h))
    for h in range(2):
        hand_over(0, 0, h, 0, False).start()
    add_inputs([own])
    cotangent(1)
    cotangent(-1)
    cotangent(2)
    cotangent(-2)
    up_take(3)
    cotangent(3)
    cotangent(-3)

    def stage_offsets(t):
        return (0,) if t == 0 else ((t, -t) if t < 4 else (4,))

    def from_sibling(t):
        for d, h, offset in x_chunks(t):
            hand_over(t, d, h, offset, True).wait_recv()
        add_inputs([other(offset) for offset in stage_offsets(t)])

    def cot_own(offsets):
        for offset in offsets:
            take_many(CT.at[mine(offset), pl.ds(0, ROWS - CAP)], cs.at[zat(offset)], cr.at[zat(offset)])
            hand_cotangent(offset, False).start()
        add_cotangents([mine(offset) for offset in offsets])

    def cot_other(offsets):
        for offset in offsets:
            hand_cotangent(offset, True).wait_recv()
        add_cotangents([other(offset) for offset in offsets])

    cot_stages = ((0, 1), (-1, 2, -2), (3, -3), (4,))
    for t in range(1, 5):
        for d, h, offset in x_chunks(t):
            ring_take(*x_ring(t, d, h))
            if t < 4 and active(t + 1, d, h):
                ring_send(*x_ring(t + 1, d, h))
            hand_over(t, d, h, offset, False).start()
        if t == 1:
            up_take(4)
            cotangent(4)
        add_inputs([mine(offset) for offset in stage_offsets(t)])
        from_sibling(t - 1)
        cot_own(cot_stages[t - 1])
        if t > 1:
            cot_other(cot_stages[t - 2])
    from_sibling(4)
    cot_other(cot_stages[3])

    def hidden(r, carry):
        rows = pl.ds(pl.multiple_of(r * 64, 64), 64)
        gate, upper, back = G[rows, 0:CH], G[rows, CH : 2 * CH], A[rows, :]
        logistic = jax.nn.sigmoid(gate)
        silu = gate * logistic
        ACT[rows, :] = (silu * upper).astype(BF16)
        gate_back = (back * upper * silu_slope(gate, logistic)).astype(BF16)
        upper_back = (back * silu).astype(BF16)
        CAT[rows, 0:CH] = gate_back
        CAT[rows, CH : 2 * CH] = upper_back
        return carry

    lax.fori_loop(0, 12, hidden, 0)

    def send_sums():
        def row_sums(r, carry):
            rows = pl.ds(pl.multiple_of(r * 64, 64), 64)
            RC[rows, :] = jnp.sum(CAT[rows, :].astype(F32) * G[rows, :], axis=1, keepdims=True)
            return carry

        lax.fori_loop(0, 12, row_sums, 0)
        slot_lane = lax.broadcasted_iota(jnp.int32, (CAP, 128), 0) == lax.broadcasted_iota(
            jnp.int32, (CAP, 128), 1
        )
        top = lax.broadcasted_iota(jnp.int32, (8, 128), 0) == 0
        for p in range(NS):
            row = jnp.sum(jnp.where(slot_lane, RC[p * CAP : p * CAP + CAP, :], 0.0), axis=0, keepdims=True)
            KS[p] = jnp.where(top, row, 0.0)

        def send(p):
            remote(KS.at[p], KR.at[sp], ks.at[0], kr.at[0], (p, tp)).start()

        each_peer(send)
        KR[sp] = KS[sp]

    def inner_sums():
        take_many(KR.at[pl.ds(0, NS - 1)], ks.at[0], kr.at[0])
        by_slot = jnp.sum(KR[...], axis=1)
        names = lax.broadcasted_iota(jnp.int32, (NS, TOK), 0)
        ranks = lax.broadcasted_iota(jnp.int32, (128, TOK), 0)
        total = jnp.zeros((1, TOK), F32)
        for k in range(2):
            picked = lax.dot_general(
                by_slot, (ranks == RK[k : k + 1, :]).astype(F32), (((1,), (0,)), ((), ())),
                precision=lax.Precision.HIGHEST, preferred_element_type=F32,
            )
            total = total + jnp.sum(
                jnp.where(names == routes_ref[k : k + 1, :], picked, 0.0), axis=0, keepdims=True
            )
        row = lax.broadcasted_iota(jnp.int32, (8, 128), 0)
        exchange_set(
            1, jnp.where(row == 0, total[:, 0:128], jnp.where(row == 4, total[:, 128:TOK], 0.0))
        )
        exchange_start(1)

    def for_sibling(offset):
        q = zat(offset)
        j = other(offset)

        SB[q] = dot(CAT[...], WC[cols(j), :], 1, 1).astype(BF16)
        remote(SB.at[q], SR.at[q], sbs.at[q], sbr.at[q], sibling).start()

    def take_sibling(offset):
        q = zat(offset)
        remote(SB.at[q], SR.at[q], sbs.at[q], sbr.at[q], sibling).wait_recv()

    def chip_part(offset):
        q = zat(offset)
        take_sibling(offset)
        part = dot(CAT[...], WC[cols(mine(offset)), :], 1, 1) + SR[q].astype(F32)
        AP[q] = part[:, 0:CH]
        PB[q] = part[:, CH : 2 * CH].astype(BF16)

        def send(p):
            remote(PB.at[q, slot_rows(p)], RB.at[q, slot_rows(sp)], bs.at[q], br.at[q], (p, tp)).start()

        each_peer(send)
        RB[q, slot_rows(sp), :] = PB[q, slot_rows(sp), :]

    def rs_copy(d, k, h):
        part = pl.ds(h * HALF, HALF)
        return remote(
            RSS.at[d, k, part], RSR.at[d, k, part], rss.at[d, k, h], rsr.at[d, k, h], zdev(1 - 2 * d)
        )

    def rs_active(k, d, h):
        return k >= 1 or d == h

    def rs_send(k, d, h):
        offset = (4 - k) * (1 - 2 * d)
        incoming = k >= 1 and rs_active(k - 1, d, h)
        if incoming:
            rs_copy(d, k - 1, h).wait_recv()

        part = slice(h * HALF, h * HALF + HALF)
        total = AP[zat(offset), part, :]
        if incoming:
            total = total + RSR[d, k - 1, part, :].astype(F32)
        RSS[d, k, part, :] = total.astype(BF16)
        rs_copy(d, k, h).start()

    def back_take(offset):
        q = zat(offset)
        take_many(RB.at[q, pl.ds(0, ROWS - CAP)], bs.at[q], br.at[q])

    def token_part(offset, h):
        return dot(PICK[:, h * CH : h * CH + CH], RB[zat(offset)], 0, 0)

    def ts_copy(d, k, h):
        part = pl.ds(h * CH, CH)
        return remote(
            TSS.at[d, k, part], TSR.at[d, k, part], tss.at[d, k, h], tsr.at[d, k, h], zdev(1 - 2 * d)
        )

    def ts_send(k, d, h):
        total = token_part((4 - k) * (1 - 2 * d), h)
        if k >= 1 and rs_active(k - 1, d, h):
            ts_copy(d, k - 1, h).wait_recv()
            total = total + TSR[d, k - 1, h * CH : h * CH + CH, :].astype(F32)
        TSS[d, k, h * CH : h * CH + CH, :] = total.astype(BF16)
        ts_copy(d, k, h).start()

    def ts_step(k):
        for offset in stage_offsets(4 - k):
            back_take(offset)
        for d, h in ((0, 1), (1, 0), (0, 0), (1, 1)):
            if rs_active(k, d, h):
                ts_send(k, d, h)

    def rs_step(k):
        for d, h in ((0, 1), (1, 0), (0, 0), (1, 1)):
            if rs_active(k, d, h):
                rs_send(k, d, h)

    def gradients(first_block):
        def step(b, carry):
            j = first_block + b
            both = dot(X[j], CAT[...], 0, 0)
            GG[cols(j), :] = both[:, 0:CH]
            GU[cols(j), :] = both[:, CH : 2 * CH]
            GD[:, cols(j)] = dot(ACT[...], CT[j], 0, 0)
            return carry

        lax.fori_loop(0, 4, step, 0)

    for_sibling(4)
    for_sibling(3)
    for_sibling(-3)
    chip_part(4)
    rs_step(0)
    chip_part(3)
    chip_part(-3)
    for_sibling(2)
    for_sibling(-2)
    rs_step(1)
    chip_part(2)
    chip_part(-2)
    for_sibling(1)
    for_sibling(-1)
    for_sibling(0)
    rs_step(2)
    send_sums()
    ts_step(0)
    chip_part(1)
    chip_part(-1)
    gradients(0)
    rs_step(3)
    inner_sums()
    chip_part(0)
    ts_step(1)
    gradients(4)
    for h in range(2):
        rs_copy(0, 3, h).wait_recv()
        rs_copy(1, 3, h).wait_recv()

        part = slice(h * HALF, h * HALF + HALF)
        FIN[part, :] = (
            AP[z, part, :] + RSR[0, 3, part, :].astype(F32) + RSR[1, 3, part, :].astype(F32)
        ).astype(BF16)

    def send_back(p):
        remote(FIN.at[slot_rows(p)], RET.at[slot_rows(sp)], fs.at[0], fr.at[0], (p, tp)).start()

    each_peer(send_back)
    RET[slot_rows(sp), :] = FIN[slot_rows(sp), :]
    ts_step(2)
    gradients(8)
    ts_step(3)
    def sg_ring(t, d, h, r, arriving):
        sign = 1 - 2 * d
        j = mine(-sign * (t if arriving else t - 1))
        block = SG.at[j, pl.ds(r * CH, CH), pl.ds(h * CH, CH)]
        return remote(block, block, sgs.at[d, t - 1, h, r], sgr.at[d, t - 1, h, r], zdev(sign))

    def sg_hand(t, d, h, offset, arriving):
        block = SG.at[other(offset) if arriving else mine(offset), :, pl.ds(h * CH, CH)]
        return remote(block, block, dgs.at[t, d, h], dgr.at[t, d, h], sibling)

    def sg_first(h, token_back):
        part = slice(h * CH, h * CH + CH)
        SG[own, :, part] = (
            UP[z, :, part].astype(F32)
            + inverse * gain_ref[:, part] * token_back
            - ST[:, part].astype(F32) * share
        ).astype(BF16)
        for r in range(2):
            for d in range(2):
                sg_ring(1, d, h, r, False).start()
        sg_hand(0, 0, h, 0, False).start()

    share = inverse * inverse * (exchange_end(1)[:, 0:1] / MODEL)
    take_many(RET.at[pl.ds(0, ROWS - CAP)], fs.at[0], fr.at[0])
    sg_first(0, dot(PICK[...], RET[...], 0, 0))
    back_take(0)
    finals = []
    for h in range(2):
        total = token_part(0, h)
        for d in range(2):
            ts_copy(d, 3, h).wait_recv()
            total = total + TSR[d, 3, h * CH : h * CH + CH, :].astype(F32)
        finals.append(total)
    sg_first(1, jnp.concatenate(finals, axis=0))
    loads[6].wait()

    def mix(j):
        block = SG[j]
        part = dot(MO[...], block, 1, 0).astype(BF16)

        @pl.when(j == sp)
        def _():
            GOR[sp] = part

        @pl.when(j != sp)
        def _():
            GOS[j] = part
            remote(GOS.at[j], GOR.at[sp], gs.at[0], gr.at[0], (j, tp)).start()

        MB[...] = MB[...] + dot(block, WO[:, cols(j)], 1, 1)

    MB[...] = jnp.zeros_like(MB)
    mix(own)

    def mix_other(t):
        for d, h, offset in x_chunks(t):
            sg_hand(t, d, h, offset, True).wait_recv()
        for offset in stage_offsets(t):
            mix(other(offset))

    for t in range(1, 5):
        for h in range(2):
            here = [(d, offset) for d, g, offset in x_chunks(t) if g == h]
            for r in range(2):
                for d, _ in here:
                    sg_ring(t, d, h, r, True).wait_recv()
                    if t < 4 and active(t + 1, d, h):
                        sg_ring(t + 1, d, h, r, False).start()
            for d, offset in here:
                sg_hand(t, d, h, offset, False).start()
        for offset in stage_offsets(t):
            mix(mine(offset))
        mix_other(t - 1)
    mix_other(4)

    scaled = SCL[...]
    norm_in = MB[...] * silu_slope(scaled, jax.nn.sigmoid(scaled)) * lng_ref[...]
    exchange_set(
        2,
        columns_to_rows([
            jnp.sum(norm_in, axis=1, keepdims=True),
            jnp.sum(norm_in * CEN[...], axis=1, keepdims=True),
        ]),
    )
    exchange_start(2)

    gradients(12)
    stores = [
        pltpu.make_async_copy(GG, gg_h, ls.at[7]),
        pltpu.make_async_copy(GU, gu_h, ls.at[8]),
        pltpu.make_async_copy(GD, gd_h, ls.at[9]),
    ]
    for store in stores:
        store.start()
    sums = exchange_end(2)
    conv_back = inv_std * (
        norm_in - sums[:, 0:1] / CHANNELS - CEN[...] * (sums[:, 1:2] / CHANNELS)
    )
    HS[...] = conv_back[0:32, :]
    previous = ((sp + NS - 1) % NS, tp)

    @pl.when(sp > 0)
    def _():
        remote(HS, HALO, hs.at[0], hr.at[0], previous).start()

    cb_o[0:TOK, :] = conv_back

    @pl.when(sp < NS - 1)
    def _():
        remote(HS, HALO, hs.at[0], hr.at[0], previous).wait_recv()
        cb_o[TOK : TOK + 32, :] = HALO[...]

    @pl.when(sp == NS - 1)
    def _():
        cb_o[TOK : TOK + 32, :] = jnp.zeros((32, CH), F32)

    take_many(GOR.at[pl.ds(0, NS - 1)], gs.at[0], gr.at[0])

    def total(i, acc):
        return acc + GOR[i].astype(F32)

    go_o[...] = lax.fori_loop(0, NS, total, jnp.zeros((CH, W), F32))

    for t in range(1, 5):
        for d, h in STEPS:
            if active(t, d, h):
                ring(UP, zat, TOK // 2, ups, upr, t, d, h, False).wait_send()
                ring(*x_ring(t, d, h), False).wait_send()
                for r in range(2):
                    sg_ring(t, d, h, r, False).wait_send()
    for t in range(5):
        for d, h, offset in x_chunks(t):
            hand_over(t, d, h, offset, False).wait_send()
            sg_hand(t, d, h, offset, False).wait_send()
    for offset in OFFSETS:
        q = zat(offset)
        flush_many(SC.at[q, pl.ds(0, ROWS - CAP)], cs.at[q], cr.at[q])
        hand_cotangent(offset, False).wait_send()
        flush_many(PB.at[q, pl.ds(0, ROWS - CAP)], bs.at[q], br.at[q])
        remote(SB.at[q], SR.at[q], sbs.at[q], sbr.at[q], sibling).wait_send()
    for k in range(4):
        for d, h in STEPS:
            if rs_active(k, d, h):
                rs_copy(d, k, h).wait_send()
                ts_copy(d, k, h).wait_send()
    for n in range(3):
        exchange_flush(n)
    flush_many(KS.at[pl.ds(0, NS - 1)], ks.at[0], kr.at[0])
    flush_many(SI.at[pl.ds(0, ROWS - CAP)], as_.at[0], ar.at[0])
    flush_many(FIN.at[pl.ds(0, ROWS - CAP)], fs.at[0], fr.at[0])
    flush_many(GOS.at[pl.ds(0, NS - 1)], gs.at[0], gr.at[0])

    @pl.when(sp > 0)
    def _():
        remote(HS, HALO, hs.at[0], hr.at[0], previous).wait_send()

    for store in stores:
        store.wait()


def last_kernel(
    gg_i, gu_i, gd_i, cb_ref, go_ref, taps_ref, value_ref, gate_ref,
    gg_o, gu_o, gd_o, vg_o, tg_o, go_o, bufs_tall, buf_wide, lsem, ssem,
):
    pieces = []
    for a, (src, dst) in enumerate(((gg_i, gg_o), (gu_i, gu_o))):
        for q in range(4):
            part = pl.ds(q * 1024, 1024)
            pieces.append((src.at[part], bufs_tall.at[a, part], dst.at[part]))
    for q in range(4):
        part = pl.ds(q * 32, 32)
        pieces.append((gd_i.at[part], buf_wide.at[part], gd_o.at[part]))
    ins = [pltpu.make_async_copy(s, b, lsem.at[n]) for n, (s, b, _) in enumerate(pieces)]
    outs = [pltpu.make_async_copy(b, d, ssem.at[n]) for n, (_, b, d) in enumerate(pieces)]
    for copy in ins:
        copy.start()
    for i, o in zip(ins, outs):
        i.wait()
        o.start()
    go_o[...] = go_ref[...]
    acc = jnp.zeros((TOK, CH), F32)
    for tap in range(TAPS):
        acc = acc + taps_ref[tap : tap + 1, :] * cb_ref[TAPS - 1 - tap : TAPS - 1 - tap + TOK, :]
    sigma = jax.nn.sigmoid(gate_ref[...].astype(F32))
    vg_o[...] = (acc * sigma).astype(BF16)
    tg_o[...] = (acc * value_ref[...].astype(F32) * sigma * (1.0 - sigma)).astype(BF16)
    for copy in outs:
        copy.wait()


def shape(dims, dtype):
    return jax.ShapeDtypeStruct(dims, dtype)


def per_device(
    upstream, stream, norm_gain, routes, route_weights, w_gate, w_up, w_down,
    value_in, gate_in, conv_pre, ln_gain, conv_taps, w_out,
):
    near, far = pl.BlockSpec(memory_space=pltpu.VMEM), pl.BlockSpec(memory_space=pl.ANY)
    dma, vm = pltpu.SemaphoreType.DMA, pltpu.VMEM
    grads = [shape((MODEL, CH), F32), shape((MODEL, CH), F32), shape((CH, MODEL), F32)]
    scratch = [
        vm((NZ, TOK, W), BF16), vm((TOK, W), BF16), vm((TOK, CH), BF16),
        vm((MODEL, 2 * CH), BF16), vm((CH, MODEL), BF16), vm((CH, MODEL), BF16),
        vm((ROWS, TOK), BF16), vm((ROWS, 1), F32),
        vm((ROWS, W), BF16), vm((NZ, ROWS, W), BF16),
        vm((NS, ROWS, W), BF16), vm((NS, ROWS, W), BF16),
        vm((ROWS, 2 * CH), F32), vm((ROWS, CH), F32),
        vm((ROWS, 2 * CH), BF16), vm((ROWS, CH), BF16),
        vm((MODEL, CH), F32), vm((MODEL, CH), F32), vm((CH, MODEL), F32),
        vm((NZ, ROWS, W), BF16), vm((NZ, ROWS, W), BF16),
        vm((2, 4, ROWS, CH), BF16), vm((2, 4, ROWS, CH), BF16),
        vm((NZ, ROWS, CH), BF16), vm((NZ, ROWS, CH), BF16),
        vm((2, 4, TOK, CH), BF16), vm((2, 4, TOK, CH), BF16),
        vm((NZ, ROWS, CH), F32), vm((8, TOK), jnp.int32), vm((ROWS, 1), F32),
        vm((NS, 8, 128), F32), vm((NS, 8, 128), F32),
        vm((ROWS, CH), BF16), vm((ROWS, CH), BF16),
        vm((NS, TOK, W), BF16), vm((TOK, CH), F32),
        vm((CH, TOK), BF16), vm((TOK, CH), F32), vm((TOK, CH), F32),
        vm((32, CH), F32), vm((32, CH), F32),
        vm((NS, CH, W), BF16), vm((NS, CH, W), BF16),
        vm((3, NS, 8, 128), F32), vm((3, 8, 128), F32),
        dma((10,)),
        dma((2, 4, 2)), dma((2, 4, 2)), dma((2, 4, 2)), dma((2, 4, 2)),
        dma((5, 2, 2)), dma((5, 2, 2)),
        dma((1,)), dma((1,)),
        dma((NZ,)), dma((NZ,)), dma((NZ,)), dma((NZ,)),
        dma((NZ,)), dma((NZ,)),
        dma((2, 4, 2)), dma((2, 4, 2)),
        dma((NZ,)), dma((NZ,)), dma((2, 4, 2)), dma((2, 4, 2)),
        dma((1,)), dma((1,)),
        dma((3,)), dma((3,)),
        dma((1,)), dma((1,)),
        dma((2, 4, 2, 2)), dma((2, 4, 2, 2)), dma((5, 2, 2)), dma((5, 2, 2)),
        dma((1,)), dma((1,)), dma((1,)), dma((1,)),
    ]
    gg, gu, gd, conv_back, out_sum = pl.pallas_call(
        comm_kernel,
        name="exchange",
        out_shape=grads + [shape((TOK + 32, CH), F32), shape((CH, W), F32)],
        in_specs=[near] * 4 + [far] * 7,
        out_specs=[far] * 3 + [near] * 2,
        scratch_shapes=scratch,
        compiler_params=pltpu.CompilerParams(
            collective_id=0, has_side_effects=True, vmem_limit_bytes=67_000_000
        ),
    )(
        norm_gain.reshape(1, W), routes.T, route_weights.T, ln_gain.reshape(1, CH),
        upstream, stream, w_gate[0], w_up[0], w_down[0], conv_pre, w_out,
    )
    grad_gate, grad_up, grad_down, value_grad, gate_grad, grad_out = pl.pallas_call(
        last_kernel,
        name="last",
        out_shape=grads + [shape((TOK, CH), BF16)] * 2 + [shape((CH, W), F32)],
        in_specs=[far] * 3 + [near] * 5,
        out_specs=[far] * 3 + [near] * 3,
        scratch_shapes=[
            vm((2, MODEL, CH), F32), vm((CH, MODEL), F32), dma((12,)), dma((12,)),
        ],
        compiler_params=pltpu.CompilerParams(vmem_limit_bytes=67_000_000),
    )(gg, gu, gd, conv_back, out_sum, conv_taps, value_in, gate_in)
    return (grad_gate[None], grad_up[None], grad_down[None], grad_out, value_grad, gate_grad)


def solution(mesh):
    return jax.shard_map(
        per_device,
        mesh=mesh,
        in_specs=(
            P("sp", "tp"), P("sp", "tp"), P("tp"), P("sp", None), P("sp", None),
            P("sp", None, "tp"), P("sp", None, "tp"), P("sp", "tp", None),
            P("sp", "tp"), P("sp", "tp"), P("sp", "tp"), P("tp"), P(None, "tp"), P("tp", None),
        ),
        out_specs=(
            P("sp", None, "tp"), P("sp", None, "tp"), P("sp", "tp", None),
            P("tp", "sp"), P("sp", "tp"), P("sp", "tp"),
        ),
        check_vma=False,
    )
```
